128 devices in a mesh: sp: 16 (over z, y), dp: 8 (over x, core).
Axes of the slice: x: 4, y: 4, z: 4, core: 2. Of those that a mesh axis runs over, the one named last changes fastest.
Arguments:
- inputs: bfloat16 [8, 3072, 2048], P('dp', 'sp'), may hold values from -6 to 6
- in_gain: float32 [2048], replicated, may hold values from 0.1 to 1.9
- w_query: bfloat16 [2048, 1024], P('dp', 'sp'), may hold values from -0.125 to 0.125
- w_key: bfloat16 [2048, 256], P('dp', 'sp'), may hold values from -0.375 to 0.375
- w_value: bfloat16 [2048, 256], P('dp', 'sp'), may hold values from -0.125 to 0.125
- key_bias: float32 [8, 3072, 16], P('dp', None, 'sp'), may hold values from -20 to 0
- out_gain: float32 [1024], replicated, may hold values from 0.1 to 1.9
- w_out: bfloat16 [1024, 2048], P('sp', 'dp'), may hold values from -0.1875 to 0.1875
Outputs:
- mixed: bfloat16 [8, 3072, 2048], P('dp', 'sp')
The draws below stay inside these ranges and needn't reach their ends.
All inputs are finite; a program needn't handle non-finite values.
Results may differ from the reference program's by a relative error of at most 0.012.
The reference program's roundings to bfloat16 on the way (of `normed`, `queries`, `keys`, `values`, `sticks` and `head_out`) count: a program that leaves them out, or rounds other values in their place, can miss the bound.
Values may be sent and summed in bfloat16 or wider, within the bound.
No kernel may reach another device: no remote copies, remote signals or barrier semaphores. Data moves between devices by JAX's collectives and lax.ppermute only.
A program may use at most 128 MiB of HBM per device.

```python
import math
import jax
import jax.numpy as jnp
from jax import lax

D = 2048
QUERY_HEADS = 16
KV_HEADS = 4
HEAD_DIM = 64
TOK_DEV = 192
SEQUENCE_LENGTH = 3072
BATCH_COUNT = 8


logit_shift = 4.5


def draw_key_bias(key, part):
    parallel_flows = jax.random.split(jax.random.fold_in(key, 17), 6)
    fast_share = 0.5
    coins = jax.random.uniform(parallel_flows[0], (BATCH_COUNT, 1, QUERY_HEADS), jnp.float32)
    fast = coins < fast_share
    fast_rate = jnp.exp(jax.random.uniform(parallel_flows[1], (BATCH_COUNT, 1, QUERY_HEADS), jnp.float32, math.log(1.0 / 100.0), math.log(1.0 / 30.0)))
    slow_rate = jnp.exp(jax.random.uniform(parallel_flows[2], (BATCH_COUNT, 1, QUERY_HEADS), jnp.float32, math.log(1.0 / (8.0 * SEQUENCE_LENGTH)), math.log(1.0 / (2.0 * SEQUENCE_LENGTH))))
    rate = jnp.where(fast, fast_rate, slow_rate)
    factor = jnp.exp(jax.random.uniform(parallel_flows[3], (BATCH_COUNT, SEQUENCE_LENGTH // TOK_DEV, QUERY_HEADS), jnp.float32, math.log(0.5), math.log(2.0)))
    factor = jnp.repeat(factor, TOK_DEV, axis=1)
    start_offsets = jnp.log(rate * factor) - logit_shift
    transfer_group_at = jax.random.randint(parallel_flows[4], (BATCH_COUNT, 4), 0, SEQUENCE_LENGTH)
    transfer_group = jnp.any(jnp.arange(SEQUENCE_LENGTH)[None, :, None] == transfer_group_at[:, None, :], axis=2)
    transfer_group_value = jax.random.uniform(parallel_flows[5], (BATCH_COUNT, SEQUENCE_LENGTH, QUERY_HEADS), jnp.float32, -4.0, -2.0)
    start_offsets = jnp.where(transfer_group[:, :, None], transfer_group_value, start_offsets)
    return start_offsets.astype(jnp.float32)


def block_scale(stream_key, extent, cuts, smallest, largest):
    def one(dim, parts):
        draws = jax.random.uniform(jax.random.fold_in(jax.random.fold_in(stream_key, 6), dim), (parts,), jnp.float32, smallest / len(cuts), largest / len(cuts))
        return jnp.repeat(jnp.exp(draws), extent[dim] // parts).reshape((-1,) + (1,) * (len(extent) - dim - 1))

    loudness = one(*cuts[0])
    for cut in cuts[1:]:
        loudness = loudness * one(*cut)
    return loudness


def gaussian(rng, shape, width, reach, cuts=(), kind=jnp.bfloat16):
    drawn = jax.random.normal(rng, shape, jnp.float32) * width
    if len(cuts) > 0:
        drawn = block_scale(rng, shape, cuts, -0.22, 0.18) * drawn
    return jnp.clip(drawn, min=-reach, max=reach).astype(kind)


def setup_inputs(seed: int = 0) -> dict:
    splits = jax.random.split(jax.random.key(seed), 9)
    inputs = gaussian(splits[0], (BATCH_COUNT, SEQUENCE_LENGTH, D), 1.0, 6.0, ((0, 8), (1, 16)))
    in_gain = jnp.clip(1.0 + 0.18 * jax.random.normal(splits[1], (D,), jnp.float32), 0.1, 1.9)
    w_query = gaussian(splits[2], (D, QUERY_HEADS * HEAD_DIM), D ** -0.5, 0.125, ((0, 8), (1, 16)))
    w_key = gaussian(splits[3], (D, KV_HEADS * HEAD_DIM), (D // 9) ** -0.5, 0.375, ((0, 8), (1, 16)))
    w_value = gaussian(splits[4], (D, KV_HEADS * HEAD_DIM), D ** -0.5, 0.125, ((0, 8), (1, 16)))
    key_bias = draw_key_bias(jax.random.fold_in(splits[8], 71), 0)
    out_gain = jnp.clip(1.0 + 0.18 * jax.random.normal(splits[6], (QUERY_HEADS * HEAD_DIM,), jnp.float32), 0.1, 1.9)
    w_out = gaussian(splits[7], (QUERY_HEADS * HEAD_DIM, D), (QUERY_HEADS * HEAD_DIM) ** -0.5, 0.1875, ((0, 16), (1, 8)))
    return dict(inputs=inputs, in_gain=in_gain, w_query=w_query, w_key=w_key, w_value=w_value, key_bias=key_bias, out_gain=out_gain, w_out=w_out)


norm_eps = 1e-06

def breaking_rows(query_rows, key_rows, value_rows, bias_row, start):
    logits = jnp.dot(query_rows, key_rows.T, preferred_element_type=jnp.float32) * HEAD_DIM ** (-0.5) + bias_row[None, :]
    rows = start + jnp.arange(query_rows.shape[0], dtype=jnp.int32)[:, None]
    columns = jnp.arange(key_rows.shape[0], dtype=jnp.int32)[None, :]
    strict = columns < rows
    log_keep = jnp.where(strict, jax.nn.log_sigmoid(-logits), jnp.float32(0.0))
    log_rest = lax.cumsum(log_keep, axis=1, reverse=True) - log_keep
    sticks = jnp.where(strict, jnp.exp(jax.nn.log_sigmoid(logits) + log_rest), jnp.float32(0.0)).astype(jnp.bfloat16)
    return jnp.dot(sticks, value_rows, preferred_element_type=jnp.float32)

def one_head(packed):
    query_all, key_all, value_all, bias_all = packed
    block = min(512, SEQUENCE_LENGTH)
    pieces = []
    for index in range(SEQUENCE_LENGTH // block):
        start = index * block
        end = start + block
        pieces.append(breaking_rows(query_all[start:end], key_all[:end], value_all[:end], bias_all[:end], start))
    return jnp.concatenate(pieces, axis=0)

def reference(inputs, in_gain, w_query, w_key, w_value, key_bias, out_gain, w_out):
    wide = inputs.astype(jnp.float32)
    normed = (wide * lax.rsqrt(lax.optimization_barrier(jnp.mean(wide * wide, axis=-1, keepdims=True)) + norm_eps) * in_gain).astype(jnp.bfloat16)
    flat = normed.reshape(BATCH_COUNT * SEQUENCE_LENGTH, D)
    queries = jnp.dot(flat, w_query, preferred_element_type=jnp.float32).astype(jnp.bfloat16)
    keys = jnp.dot(flat, w_key, preferred_element_type=jnp.float32).astype(jnp.bfloat16)
    values = jnp.dot(flat, w_value, preferred_element_type=jnp.float32).astype(jnp.bfloat16)
    group = QUERY_HEADS // KV_HEADS
    queries = queries.reshape(BATCH_COUNT, SEQUENCE_LENGTH, QUERY_HEADS, HEAD_DIM).transpose(0, 2, 1, 3).reshape(BATCH_COUNT * QUERY_HEADS, SEQUENCE_LENGTH, HEAD_DIM)
    keys = jnp.repeat(keys.reshape(BATCH_COUNT, SEQUENCE_LENGTH, KV_HEADS, HEAD_DIM), group, axis=2)
    keys = keys.transpose(0, 2, 1, 3).reshape(BATCH_COUNT * QUERY_HEADS, SEQUENCE_LENGTH, HEAD_DIM)
    values = jnp.repeat(values.reshape(BATCH_COUNT, SEQUENCE_LENGTH, KV_HEADS, HEAD_DIM), group, axis=2)
    values = values.transpose(0, 2, 1, 3).reshape(BATCH_COUNT * QUERY_HEADS, SEQUENCE_LENGTH, HEAD_DIM)
    biases = key_bias.transpose(0, 2, 1).reshape(BATCH_COUNT * QUERY_HEADS, SEQUENCE_LENGTH)
    attended = lax.map(one_head, (queries, keys, values, biases))
    attended = attended.reshape(BATCH_COUNT, QUERY_HEADS, SEQUENCE_LENGTH, HEAD_DIM).transpose(0, 2, 1, 3)
    scaled = attended * lax.rsqrt(lax.optimization_barrier(jnp.mean(attended * attended, axis=-1, keepdims=True)) + norm_eps)
    head_out = (scaled * out_gain.reshape(QUERY_HEADS, HEAD_DIM)).astype(jnp.bfloat16).reshape(BATCH_COUNT * SEQUENCE_LENGTH, QUERY_HEADS * HEAD_DIM)
    mixed = jnp.dot(head_out, w_out, preferred_element_type=jnp.float32).astype(jnp.bfloat16)
    return mixed.reshape(BATCH_COUNT, SEQUENCE_LENGTH, D)
```

```python
import functools
import math

import jax
import jax.numpy as jnp
from jax import lax
from jax.experimental import pallas as pl
from jax.experimental.pallas import tpu as pltpu
from jax.sharding import PartitionSpec as P

HEAD_DIM = 64
LOG2E = math.log2(math.e)
norm_eps = 1e-06
SIDE = 4
HOPS = (0, 1, 3, 2)


VMEM = pl.BlockSpec(memory_space=pltpu.VMEM)
SMEM = pl.BlockSpec(memory_space=pltpu.SMEM)


def along_x(k):
    return [(i, (i + 2 * k) % (2 * SIDE)) for i in range(2 * SIDE)]


def other_core():
    return [(i, i ^ 1) for i in range(2 * SIDE)]


def along_zy(dz, dy):
    return [
        (s, ((s // SIDE + dz) % SIDE) * SIDE + (s % SIDE + dy) % SIDE) for s in range(SIDE * SIDE)
    ]


def pack_kernel(wq_ref, wk_ref, wv_ref, wo_ref, out_ref):
    wide = jnp.concatenate([wq_ref[...], wk_ref[...], wv_ref[...]], axis=1).astype(jnp.float32)
    cols = wide.shape[1]
    wide = jnp.concatenate([wide, jnp.zeros((wide.shape[0], 128 - cols), jnp.float32)], axis=1)
    out_ref[:cols, :] = wide.T[:cols, :].astype(jnp.bfloat16)
    out_ref[cols:, :] = wo_ref[...]


def project_kernel(where_ref, normed_ref, own_ref, far_ref, out_ref, order_ref, sums_ref):
    bf = jnp.bfloat16
    x, c, z, y = (where_ref[i] for i in range(4))
    rows = normed_ref.shape[0]
    for i in range(SIDE):
        for cc in range(2):
            chunk = 2 * lax.rem(x + SIDE - HOPS[i], SIDE) + lax.rem(c + cc, 2)
            order_ref[:, (2 * i + cc) * 256 : (2 * i + cc + 1) * 256] = normed_ref[
                :, pl.ds(pl.multiple_of(chunk * 256, 256), 256)
            ]
    for iz in range(SIDE):
        parts = []
        for i in range(SIDE):
            for ref in (own_ref, far_ref):
                if i < 2:
                    parts.append(jnp.concatenate([ref[0, iz, iy, i] for iy in range(SIDE)], axis=0))
                else:
                    parts.append(jnp.concatenate([ref[1, iy, iz, i - 2] for iy in range(SIDE)], axis=0))
        weights = jnp.concatenate(parts, axis=1)
        total = lax.dot_general(
            weights, order_ref[...], (((1,), (1,)), ((), ())), preferred_element_type=jnp.float32
        )
        for iy in range(SIDE):
            place = SIDE * lax.rem(z + SIDE - HOPS[iz], SIDE) + lax.rem(y + SIDE - HOPS[iy], SIDE)
            sums_ref[place] = total[96 * iy : 96 * (iy + 1), :]
    half = rows // 2
    for g in range(SIDE):
        key = jnp.concatenate([sums_ref[SIDE * g + j, 64:80, :] for j in range(SIDE)], axis=0)
        value = jnp.concatenate([sums_ref[SIDE * g + j, 80:96, :] for j in range(SIDE)], axis=0)
        turned = value.T.astype(bf)
        for j in range(SIDE):
            h = SIDE * g + j
            both = jnp.concatenate([sums_ref[h, :64, :], key], axis=0)
            out_ref[h, :rows, :] = both.T.astype(bf)
            out_ref[h, rows:, :] = jnp.concatenate([turned[:half], turned[half:]], axis=1)


def attend_kernel(got_ref, bias_ref, gain_ref, out_ref, qa_ref, kt_ref, v_ref, acc_ref, car_ref, *, src, rows, bq, bk):
    bf = jnp.bfloat16
    half = rows // 2
    length = src * rows
    lane = lax.broadcasted_iota(jnp.int32, (rows, 128), 1)
    ones = jnp.where(lane < 3, 1.0, 0.0).astype(bf)
    for b in range(src):
        both = got_ref[b, :rows, :]
        wide = both[:, :HEAD_DIM].astype(jnp.float32) * (LOG2E * HEAD_DIM ** -0.5)
        high = wide.astype(bf)
        low = (wide - high.astype(jnp.float32)).astype(bf)
        qa_ref[b * rows : (b + 1) * rows, :128] = jnp.concatenate([high, low], axis=1)
        qa_ref[b * rows : (b + 1) * rows, 128:] = ones
        vv = got_ref[b, rows:, :]
        v_ref[b * rows : b * rows + half, :] = vv[:, :HEAD_DIM]
        v_ref[b * rows + half : (b + 1) * rows, :] = vv[:, HEAD_DIM:]
    step = 2 * rows
    for b in range(src // 2):
        pair = jnp.concatenate([got_ref[2 * b, :rows, :], got_ref[2 * b + 1, :rows, :]], axis=0)
        kt = pair.astype(jnp.float32).T[HEAD_DIM:, :].astype(bf)
        kt_ref[:HEAD_DIM, b * step : (b + 1) * step] = kt
        kt_ref[HEAD_DIM : 2 * HEAD_DIM, b * step : (b + 1) * step] = kt
    b2 = bias_ref[...] * LOG2E
    b_high = b2.astype(bf).astype(jnp.float32)
    b_mid = (b2 - b_high).astype(bf).astype(jnp.float32)
    b_low = b2 - b_high - b_mid
    row = lax.broadcasted_iota(jnp.int32, (128, length), 0)
    tail = jnp.where(row == 0, b_high, jnp.where(row == 1, b_mid, jnp.where(row == 2, b_low, 0.0)))
    kt_ref[2 * HEAD_DIM :, :] = tail.astype(bf)

    tri = (
        lax.broadcasted_iota(jnp.int32, (bk, bk), 0) > lax.broadcasted_iota(jnp.int32, (bk, bk), 1)
    ).astype(bf)

    def tile(row0, nrows, acc0, col0, masked):
        x = jnp.dot(
            qa_ref[pl.ds(row0, nrows), :], kt_ref[:, pl.ds(col0, bk)], preferred_element_type=jnp.float32
        )
        soft = jnp.maximum(x, jnp.log2(1.0 + jnp.exp2(jnp.minimum(x, 126.0))))
        own = x - soft
        if masked:
            keep = lax.broadcasted_iota(jnp.int32, (nrows, bk), 1) < lax.broadcasted_iota(
                jnp.int32, (nrows, bk), 0
            )
            soft = jnp.where(keep, soft, 0.0)
        after = jnp.dot(soft.astype(bf), tri, preferred_element_type=jnp.float32)
        carry = car_ref[acc0 : acc0 + nrows, :]
        a = jnp.exp2(own - after - jnp.concatenate([carry] * (bk // 128), axis=1))
        if masked:
            a = jnp.where(keep, a, 0.0)
        acc_ref[acc0 : acc0 + nrows, :] += jnp.dot(
            a.astype(bf), v_ref[pl.ds(col0, bk), :], preferred_element_type=jnp.float32
        )
        car_ref[acc0 : acc0 + nrows, :] = carry + jnp.broadcast_to((after + soft)[:, :1], (nrows, 128))

    per = bq // bk
    quarter = rows // 2

    def q_tile(i, _):
        base = pl.multiple_of(i * bq, bq)
        acc_ref[...] = jnp.zeros_like(acc_ref)
        car_ref[...] = jnp.zeros_like(car_ref)
        for c in reversed(range(per)):
            for r in range(c, per):
                tile(base + r * bk, bk, r * bk, base + c * bk, r == c)

        def k_tile(j, _):
            col = pl.multiple_of((i - 1 - j) * bq, bq)
            for c in reversed(range(per)):
                tile(base, bq, 0, col + c * bk, False)
            return 0

        lax.fori_loop(0, i, k_tile, 0)
        att = acc_ref[...]
        scaled = att * lax.rsqrt(jnp.mean(att * att, axis=1, keepdims=True) + norm_eps) * gain_ref[...]
        head = scaled.astype(bf)
        count = bq // quarter
        for p in range(count // 2):
            out_ref[pl.ds(i * (count // 2) + p, 1)] = jnp.concatenate(
                [head[2 * p * quarter : (2 * p + 1) * quarter], head[(2 * p + 1) * quarter : (2 * p + 2) * quarter]],
                axis=1,
            )[None]
        return 0

    lax.fori_loop(0, length // bq, q_tile, 0)


def output_kernel(where_ref, got_ref, own_ref, far_ref, out_ref, heads_ref):
    x, c, z, y = (where_ref[i] for i in range(4))
    half = got_ref.shape[1]
    for iz in range(SIDE):
        for iy in range(SIDE):
            place = SIDE * lax.rem(z + SIDE - HOPS[iz], SIDE) + lax.rem(y + SIDE - HOPS[iy], SIDE)
            block = got_ref[place]
            at = (SIDE * iz + iy) * HEAD_DIM
            heads_ref[:half, at : at + HEAD_DIM] = block[:, :HEAD_DIM]
            heads_ref[half:, at : at + HEAD_DIM] = block[:, HEAD_DIM:]
    for i in range(SIDE):
        for cc, ref in ((0, own_ref), (1, far_ref)):
            parts = []
            for iz in range(SIDE):
                for iy in range(SIDE):
                    parts.append(ref[0, iz, iy, i] if i < 2 else ref[1, iy, iz, i - 2])
            mixed = jnp.dot(
                heads_ref[...], jnp.concatenate(parts, axis=0), preferred_element_type=jnp.float32
            )
            chunk = 2 * lax.rem(x + SIDE - HOPS[i], SIDE) + lax.rem(c + cc, 2)
            out_ref[:, pl.ds(pl.multiple_of(chunk * 256, 256), 256)] = mixed.astype(jnp.bfloat16)


def body(inputs, in_gain, w_query, w_key, w_value, key_bias, out_gain, w_out):
    bf = jnp.bfloat16
    rows, width = inputs.shape[1], inputs.shape[2]
    sp_size = lax.axis_size("sp")
    sp, dp = lax.axis_index("sp"), lax.axis_index("dp")
    where = jnp.stack([dp // 2, dp % 2, sp // SIDE, sp % SIDE]).astype(jnp.int32)

    wide = inputs[0].astype(jnp.float32)
    normed = (
        wide * lax.rsqrt(jnp.mean(wide * wide, axis=-1, keepdims=True) + norm_eps) * in_gain
    ).astype(bf)

    piece = pl.pallas_call(
        pack_kernel,
        out_shape=jax.ShapeDtypeStruct((160, 256), bf),
        in_specs=[VMEM] * 4,
        out_specs=VMEM,
        name="pack",
    )(w_query, w_key, w_value, w_out)

    def spread(perm_of, a, axis):
        return [a] + [lax.ppermute(a, axis, perm_of(k)) for k in HOPS[1:]]

    four = jnp.stack(spread(along_x, piece, "dp"))
    first_a = jnp.stack(spread(lambda k: along_zy(0, k), four[:2], "sp"))
    first_b = jnp.stack(spread(lambda k: along_zy(k, 0), four[2:], "sp"))

    def second(lo, hi):
        a = spread(lambda k: along_zy(k, 0), first_a[:, :, lo:hi], "sp")
        b = spread(lambda k: along_zy(0, k), first_b[:, :, lo:hi], "sp")
        own = jnp.stack([jnp.stack(a), jnp.stack(b)])
        return own, lax.ppermute(own, "dp", other_core())

    own, far = second(0, 96)
    packed = pl.pallas_call(
        project_kernel,
        out_shape=jax.ShapeDtypeStruct((sp_size, rows + rows // 2, 128), bf),
        in_specs=[SMEM] + [VMEM] * 3,
        out_specs=VMEM,
        scratch_shapes=[pltpu.VMEM((rows, width), bf), pltpu.VMEM((sp_size, 96, rows), jnp.float32)],
        name="project",
    )(where, normed, own, far)
    own_out, far_out = second(96, 160)

    got = lax.all_to_all(packed, "sp", split_axis=0, concat_axis=0, tiled=True)
    gains = lax.dynamic_slice_in_dim(out_gain, sp * HEAD_DIM, HEAD_DIM, 0)[None]
    length = sp_size * rows
    bq, bk = 768, 256
    heads = pl.pallas_call(
        functools.partial(attend_kernel, src=sp_size, rows=rows, bq=bq, bk=bk),
        out_shape=jax.ShapeDtypeStruct((sp_size, rows // 2, 128), bf),
        in_specs=[VMEM] * 3,
        out_specs=VMEM,
        scratch_shapes=[
            pltpu.VMEM((length, 256), bf),
            pltpu.VMEM((256, length), bf),
            pltpu.VMEM((length, HEAD_DIM), bf),
            pltpu.VMEM((bq, HEAD_DIM), jnp.float32),
            pltpu.VMEM((bq, 128), jnp.float32),
        ],
        name="attend",
    )(got, key_bias.reshape(1, length), gains)
    returned = lax.all_to_all(heads, "sp", split_axis=0, concat_axis=0, tiled=True)
    mixed = pl.pallas_call(
        output_kernel,
        out_shape=jax.ShapeDtypeStruct((rows, width), bf),
        in_specs=[SMEM] + [VMEM] * 3,
        out_specs=VMEM,
        scratch_shapes=[pltpu.VMEM((rows, sp_size * HEAD_DIM), bf)],
        name="output",
    )(where, returned, own_out, far_out)
    return mixed[None]


def solution(mesh):
    placed = (
        P("dp", "sp", None),
        P(),
        P("dp", "sp"),
        P("dp", "sp"),
        P("dp", "sp"),
        P("dp", None, "sp"),
        P(),
        P("sp", "dp"),
    )
    return jax.shard_map(
        body, mesh=mesh, in_specs=placed, out_specs=P("dp", "sp", None), check_vma=False
    )
```

```python
import functools
import math

import jax
import jax.numpy as jnp
from jax import lax
from jax.experimental import pallas as pl
from jax.experimental.pallas import tpu as pltpu
from jax.sharding import PartitionSpec as P

HEAD_DIM = 64
LOG2E = math.log2(math.e)
norm_eps = 1e-06
SIDE = 4
HOPS = (0, 1, 3, 2)


VMEM = pl.BlockSpec(memory_space=pltpu.VMEM)


def along_x(k):
    return [(i, (i + 2 * k) % (2 * SIDE)) for i in range(2 * SIDE)]


def other_core():
    return [(i, i ^ 1) for i in range(2 * SIDE)]


def along_zy(dz, dy):
    return [
        (s, ((s // SIDE + dz) % SIDE) * SIDE + (s % SIDE + dy) % SIDE) for s in range(SIDE * SIDE)
    ]


def place_of():
    dp, sp = lax.axis_index("dp"), lax.axis_index("sp")
    return lax.div(dp, 2), lax.rem(dp, 2), lax.div(sp, SIDE), lax.rem(sp, SIDE)


def project_kernel(normed_ref, own_a, own_b, far_a, far_b, out_ref, order_ref, sums_ref):
    bf = jnp.bfloat16
    x, c, z, y = place_of()
    rows = normed_ref.shape[0]
    for i in range(SIDE):
        for cc in range(2):
            chunk = 2 * lax.rem(x + SIDE - HOPS[i], SIDE) + lax.rem(c + cc, 2)
            order_ref[:, (2 * i + cc) * 256 : (2 * i + cc + 1) * 256] = normed_ref[
                :, pl.ds(pl.multiple_of(chunk * 256, 256), 256)
            ]
    for iz in range(SIDE):
        parts = []
        for i in range(SIDE):
            for ref_a, ref_b in ((own_a, own_b), (far_a, far_b)):
                if i < 2:
                    parts.append(jnp.concatenate([ref_a[iz, iy, i] for iy in range(SIDE)], axis=0))
                else:
                    parts.append(jnp.concatenate([ref_b[iy, iz, i - 2] for iy in range(SIDE)], axis=0))
        weights = jnp.concatenate(parts, axis=1)
        total = lax.dot_general(
            weights, order_ref[...], (((1,), (1,)), ((), ())), preferred_element_type=jnp.float32
        )
        for iy in range(SIDE):
            place = SIDE * lax.rem(z + SIDE - HOPS[iz], SIDE) + lax.rem(y + SIDE - HOPS[iy], SIDE)
            sums_ref[place] = total[96 * iy : 96 * (iy + 1), :]
    half = rows // 2
    for g in range(SIDE):
        key = jnp.concatenate([sums_ref[SIDE * g + j, 64:80, :] for j in range(SIDE)], axis=0)
        value = jnp.concatenate([sums_ref[SIDE * g + j, 80:96, :] for j in range(SIDE)], axis=0)
        turned = value.T.astype(bf)
        for j in range(SIDE):
            h = SIDE * g + j
            both = jnp.concatenate([sums_ref[h, :64, :], key], axis=0)
            out_ref[h, :rows, :] = both.T.astype(bf)
            out_ref[h, rows:, :] = jnp.concatenate([turned[:half], turned[half:]], axis=1)


def attend_kernel(got_ref, bias_ref, gain_ref, out_ref, qa_ref, kt_ref, v_ref, acc_ref, car_ref, *, src, rows, bq, bk):
    bf = jnp.bfloat16
    half = rows // 2
    length = src * rows
    lane = lax.broadcasted_iota(jnp.int32, (rows, 128), 1)
    ones = jnp.where(lane < 3, 1.0, 0.0).astype(bf)
    for b in range(src):
        both = got_ref[b, :rows, :]
        wide = both[:, :HEAD_DIM].astype(jnp.float32) * (LOG2E * HEAD_DIM ** -0.5)
        high = wide.astype(bf)
        low = (wide - high.astype(jnp.float32)).astype(bf)
        qa_ref[b * rows : (b + 1) * rows, :128] = jnp.concatenate([high, low], axis=1)
        qa_ref[b * rows : (b + 1) * rows, 128:] = ones
        vv = got_ref[b, rows:, :]
        v_ref[b * rows : b * rows + half, :] = vv[:, :HEAD_DIM]
        v_ref[b * rows + half : (b + 1) * rows, :] = vv[:, HEAD_DIM:]
    step = 2 * rows
    for b in range(src // 2):
        pair = jnp.concatenate([got_ref[2 * b, :rows, :], got_ref[2 * b + 1, :rows, :]], axis=0)
        kt = pair.astype(jnp.float32).T[HEAD_DIM:, :].astype(bf)
        kt_ref[:HEAD_DIM, b * step : (b + 1) * step] = kt
        kt_ref[HEAD_DIM : 2 * HEAD_DIM, b * step : (b + 1) * step] = kt
    b2 = bias_ref[...] * LOG2E
    b_high = b2.astype(bf).astype(jnp.float32)
    b_mid = (b2 - b_high).astype(bf).astype(jnp.float32)
    b_low = b2 - b_high - b_mid
    row = lax.broadcasted_iota(jnp.int32, (128, length), 0)
    tail = jnp.where(row == 0, b_high, jnp.where(row == 1, b_mid, jnp.where(row == 2, b_low, 0.0)))
    kt_ref[2 * HEAD_DIM :, :] = tail.astype(bf)

    tri = (
        lax.broadcasted_iota(jnp.int32, (bk, bk), 0) > lax.broadcasted_iota(jnp.int32, (bk, bk), 1)
    ).astype(bf)

    def tile(row0, nrows, acc0, col0, masked):
        x = jnp.dot(
            qa_ref[pl.ds(row0, nrows), :], kt_ref[:, pl.ds(col0, bk)], preferred_element_type=jnp.float32
        )
        soft = jnp.maximum(x, jnp.log2(1.0 + jnp.exp2(jnp.minimum(x, 126.0))))
        own = x - soft
        if masked:
            keep = lax.broadcasted_iota(jnp.int32, (nrows, bk), 1) < lax.broadcasted_iota(
                jnp.int32, (nrows, bk), 0
            )
            soft = jnp.where(keep, soft, 0.0)
        after = jnp.dot(soft.astype(bf), tri, preferred_element_type=jnp.float32)
        carry = car_ref[acc0 : acc0 + nrows, :]
        a = jnp.exp2(own - after - jnp.concatenate([carry] * (bk // 128), axis=1))
        if masked:
            a = jnp.where(keep, a, 0.0)
        acc_ref[acc0 : acc0 + nrows, :] += jnp.dot(
            a.astype(bf), v_ref[pl.ds(col0, bk), :], preferred_element_type=jnp.float32
        )
        car_ref[acc0 : acc0 + nrows, :] = carry + jnp.broadcast_to((after + soft)[:, :1], (nrows, 128))

    per = bq // bk
    quarter = rows // 2

    def q_tile(i, _):
        base = pl.multiple_of(i * bq, bq)
        acc_ref[...] = jnp.zeros_like(acc_ref)
        car_ref[...] = jnp.zeros_like(car_ref)
        for c in reversed(range(per)):
            for r in range(c, per):
                tile(base + r * bk, bk, r * bk, base + c * bk, r == c)

        def k_tile(j, _):
            col = pl.multiple_of((i - 1 - j) * bq, bq)
            for c in reversed(range(per)):
                tile(base, bq, 0, col + c * bk, False)
            return 0

        lax.fori_loop(0, i, k_tile, 0)
        att = acc_ref[...]
        scaled = att * lax.rsqrt(jnp.mean(att * att, axis=1, keepdims=True) + norm_eps) * gain_ref[...]
        head = scaled.astype(bf)
        count = bq // quarter
        for p in range(count // 2):
            out_ref[pl.ds(i * (count // 2) + p, 1)] = jnp.concatenate(
                [head[2 * p * quarter : (2 * p + 1) * quarter], head[(2 * p + 1) * quarter : (2 * p + 2) * quarter]],
                axis=1,
            )[None]
        return 0

    lax.fori_loop(0, length // bq, q_tile, 0)


def output_kernel(got_ref, own_ref, far_ref, out_ref, heads_ref):
    x, c, z, y = place_of()
    half = got_ref.shape[1]
    for iz in range(SIDE):
        for iy in range(SIDE):
            place = SIDE * lax.rem(z + SIDE - HOPS[iz], SIDE) + lax.rem(y + SIDE - HOPS[iy], SIDE)
            block = got_ref[place]
            at = (SIDE * iz + iy) * HEAD_DIM
            heads_ref[:half, at : at + HEAD_DIM] = block[:, :HEAD_DIM]
            heads_ref[half:, at : at + HEAD_DIM] = block[:, HEAD_DIM:]
    for i in range(SIDE):
        for cc, ref in ((0, own_ref), (1, far_ref)):
            parts = []
            for iz in range(SIDE):
                for iy in range(SIDE):
                    parts.append(ref[i, iz, iy])
            mixed = jnp.dot(
                heads_ref[...], jnp.concatenate(parts, axis=0), preferred_element_type=jnp.float32
            )
            chunk = 2 * lax.rem(x + SIDE - HOPS[i], SIDE) + lax.rem(c + cc, 2)
            out_ref[:, pl.ds(pl.multiple_of(chunk * 256, 256), 256)] = mixed.astype(jnp.bfloat16)


def body(inputs, in_gain, w_query, w_key, w_value, key_bias, out_gain, w_out):
    bf = jnp.bfloat16
    rows, width = inputs.shape[1], inputs.shape[2]
    sp_size = lax.axis_size("sp")
    sp = lax.axis_index("sp")

    wide = inputs[0].astype(jnp.float32)
    normed = (
        wide * lax.rsqrt(jnp.mean(wide * wide, axis=-1, keepdims=True) + norm_eps) * in_gain
    ).astype(bf)

    def spread(perm_of, a, axis):
        return [a] + [lax.ppermute(a, axis, perm_of(k)) for k in HOPS[1:]]

    piece = jnp.concatenate([w_query.T, w_key.T, w_value.T], axis=0)
    four = jnp.stack(spread(along_x, piece, "dp"))
    rest_y = jnp.stack(spread(lambda k: along_zy(0, k), w_out, "sp"))
    first_a = jnp.stack(spread(lambda k: along_zy(0, k), four[:2], "sp"))
    together = jnp.concatenate([four[2:].reshape(192, 256), rest_y.reshape(256, 256)], axis=0)
    first_b = jnp.stack(spread(lambda k: along_zy(k, 0), together, "sp"))
    rest_z = first_b[:, 192:].reshape(SIDE, SIDE, 64, 256)
    first_b = first_b[:, :192].reshape(SIDE, 2, 96, 256)
    first_a, first_b, normed = lax.optimization_barrier((first_a, first_b, normed))
    own_a = spread(lambda k: along_zy(k, 0), first_a, "sp")
    own_b = spread(lambda k: along_zy(0, k), first_b, "sp")
    own_a, own_b = jnp.stack(own_a), jnp.stack(own_b)
    far_a = lax.ppermute(own_a, "dp", other_core())
    far_b = lax.ppermute(own_b, "dp", other_core())
    packed = pl.pallas_call(
        project_kernel,
        out_shape=jax.ShapeDtypeStruct((sp_size, rows + rows // 2, 128), bf),
        in_specs=[VMEM] * 5,
        out_specs=VMEM,
        scratch_shapes=[pltpu.VMEM((rows, width), bf), pltpu.VMEM((sp_size, 96, rows), jnp.float32)],
        name="project",
    )(normed, own_a, own_b, far_a, far_b)
    packed, rest_z = lax.optimization_barrier((packed, rest_z))
    rest_x = spread(along_x, rest_z, "dp")

    got = lax.all_to_all(packed, "sp", split_axis=0, concat_axis=0, tiled=True)
    gains = lax.dynamic_slice_in_dim(out_gain, sp * HEAD_DIM, HEAD_DIM, 0)[None]
    length = sp_size * rows
    bq, bk = 768, 256
    heads = pl.pallas_call(
        functools.partial(attend_kernel, src=sp_size, rows=rows, bq=bq, bk=bk),
        out_shape=jax.ShapeDtypeStruct((sp_size, rows // 2, 128), bf),
        in_specs=[VMEM] * 3,
        out_specs=VMEM,
        scratch_shapes=[
            pltpu.VMEM((length, 256), bf),
            pltpu.VMEM((256, length), bf),
            pltpu.VMEM((length, HEAD_DIM), bf),
            pltpu.VMEM((bq, HEAD_DIM), jnp.float32),
            pltpu.VMEM((bq, 128), jnp.float32),
        ],
        name="attend",
    )(got, key_bias.reshape(1, length), gains)
    heads, rest_x = lax.optimization_barrier((heads, rest_x))
    own_out = jnp.stack(rest_x)
    far_out = lax.ppermute(own_out, "dp", other_core())
    returned = lax.all_to_all(heads, "sp", split_axis=0, concat_axis=0, tiled=True)
    mixed = pl.pallas_call(
        output_kernel,
        out_shape=jax.ShapeDtypeStruct((rows, width), bf),
        in_specs=[VMEM] * 3,
        out_specs=VMEM,
        scratch_shapes=[pltpu.VMEM((rows, sp_size * HEAD_DIM), bf)],
        name="output",
    )(returned, own_out, far_out)
    return mixed[None]


def solution(mesh):
    placed = (
        P("dp", "sp", None),
        P(),
        P("dp", "sp"),
        P("dp", "sp"),
        P("dp", "sp"),
        P("dp", None, "sp"),
        P(),
        P("sp", "dp"),
    )
    return jax.shard_map(
        body, mesh=mesh, in_specs=placed, out_specs=P("dp", "sp", None), check_vma=False
    )
```

```python
import functools
import math

import jax
import jax.numpy as jnp
from jax import lax
from jax.experimental import pallas as pl
from jax.experimental.pallas import tpu as pltpu
from jax.sharding import PartitionSpec as P

HEAD_DIM = 64
LOG2E = math.log2(math.e)
norm_eps = 1e-06
SIDE = 4
HOPS = (0, 1, 3, 2)


VMEM = pl.BlockSpec(memory_space=pltpu.VMEM)


def along_x(k):
    return [(i, (i + 2 * k) % (2 * SIDE)) for i in range(2 * SIDE)]


def other_core():
    return [(i, i ^ 1) for i in range(2 * SIDE)]


def along_zy(dz, dy):
    return [
        (s, ((s // SIDE + dz) % SIDE) * SIDE + (s % SIDE + dy) % SIDE) for s in range(SIDE * SIDE)
    ]


def near(*arrays):
    return [pltpu.with_memory_space_constraint(a, pltpu.VMEM) for a in arrays]


def place_of():
    dp, sp = lax.axis_index("dp"), lax.axis_index("sp")
    return lax.div(dp, 2), lax.rem(dp, 2), lax.div(sp, SIDE), lax.rem(sp, SIDE)


def project_kernel(normed_ref, own_a, own_b, far_a, far_b, out_ref, order_ref, sums_ref):
    bf = jnp.bfloat16
    x, c, z, y = place_of()
    rows = normed_ref.shape[0]
    for i in range(SIDE):
        for cc in range(2):
            chunk = 2 * lax.rem(x + SIDE - HOPS[i], SIDE) + lax.rem(c + cc, 2)
            order_ref[:, (2 * i + cc) * 256 : (2 * i + cc + 1) * 256] = normed_ref[
                :, pl.ds(pl.multiple_of(chunk * 256, 256), 256)
            ]
    for iz in range(SIDE):
        parts = []
        for i in range(SIDE):
            for ref_a, ref_b in ((own_a, own_b), (far_a, far_b)):
                if i < 2:
                    parts.append(jnp.concatenate([ref_a[iz, iy, i] for iy in range(SIDE)], axis=0))
                else:
                    parts.append(jnp.concatenate([ref_b[iy, iz, i - 2] for iy in range(SIDE)], axis=0))
        weights = jnp.concatenate(parts, axis=1)
        total = lax.dot_general(
            weights, order_ref[...], (((1,), (1,)), ((), ())), preferred_element_type=jnp.float32
        )
        for iy in range(SIDE):
            place = SIDE * lax.rem(z + SIDE - HOPS[iz], SIDE) + lax.rem(y + SIDE - HOPS[iy], SIDE)
            sums_ref[place] = total[96 * iy : 96 * (iy + 1), :]
    half = rows // 2
    for g in range(SIDE):
        key = jnp.concatenate([sums_ref[SIDE * g + j, 64:80, :] for j in range(SIDE)], axis=0)
        value = jnp.concatenate([sums_ref[SIDE * g + j, 80:96, :] for j in range(SIDE)], axis=0)
        turned = value.T.astype(bf)
        for j in range(SIDE):
            h = SIDE * g + j
            both = jnp.concatenate([sums_ref[h, :64, :], key], axis=0)
            out_ref[h, :rows, :] = both.T.astype(bf)
            out_ref[h, rows:, :] = jnp.concatenate([turned[:half], turned[half:]], axis=1)


def attend_kernel(got_ref, bias_ref, gain_ref, out_ref, qa_ref, kt_ref, v_ref, acc_ref, car_ref, *, src, rows, bq, bk):
    bf = jnp.bfloat16
    half = rows // 2
    length = src * rows
    lane = lax.broadcasted_iota(jnp.int32, (rows, 128), 1)
    ones = jnp.where(lane < 3, 1.0, 0.0).astype(bf)
    for b in range(src):
        both = got_ref[b, :rows, :]
        wide = both[:, :HEAD_DIM].astype(jnp.float32) * (LOG2E * HEAD_DIM ** -0.5)
        high = wide.astype(bf)
        low = (wide - high.astype(jnp.float32)).astype(bf)
        qa_ref[b * rows : (b + 1) * rows, :128] = jnp.concatenate([high, low], axis=1)
        qa_ref[b * rows : (b + 1) * rows, 128:] = ones
        vv = got_ref[b, rows:, :]
        v_ref[b * rows : b * rows + half, :] = vv[:, :HEAD_DIM]
        v_ref[b * rows + half : (b + 1) * rows, :] = vv[:, HEAD_DIM:]
    step = 2 * rows
    for b in range(src // 2):
        pair = jnp.concatenate([got_ref[2 * b, :rows, :], got_ref[2 * b + 1, :rows, :]], axis=0)
        kt = pair.astype(jnp.float32).T[HEAD_DIM:, :].astype(bf)
        kt_ref[:HEAD_DIM, b * step : (b + 1) * step] = kt
        kt_ref[HEAD_DIM : 2 * HEAD_DIM, b * step : (b + 1) * step] = kt
    b2 = bias_ref[...] * LOG2E
    b_high = b2.astype(bf).astype(jnp.float32)
    b_mid = (b2 - b_high).astype(bf).astype(jnp.float32)
    b_low = b2 - b_high - b_mid
    row = lax.broadcasted_iota(jnp.int32, (128, length), 0)
    tail = jnp.where(row == 0, b_high, jnp.where(row == 1, b_mid, jnp.where(row == 2, b_low, 0.0)))
    kt_ref[2 * HEAD_DIM :, :] = tail.astype(bf)

    tri = (
        lax.broadcasted_iota(jnp.int32, (bk, bk), 0) > lax.broadcasted_iota(jnp.int32, (bk, bk), 1)
    ).astype(bf)

    def tile(row0, nrows, acc0, col0, masked):
        x = jnp.dot(
            qa_ref[pl.ds(row0, nrows), :], kt_ref[:, pl.ds(col0, bk)], preferred_element_type=jnp.float32
        )
        soft = jnp.maximum(x, jnp.log2(1.0 + jnp.exp2(jnp.minimum(x, 126.0))))
        own = x - soft
        if masked:
            keep = lax.broadcasted_iota(jnp.int32, (nrows, bk), 1) < lax.broadcasted_iota(
                jnp.int32, (nrows, bk), 0
            )
            soft = jnp.where(keep, soft, 0.0)
        after = jnp.dot(soft.astype(bf), tri, preferred_element_type=jnp.float32)
        carry = car_ref[acc0 : acc0 + nrows, :]
        a = jnp.exp2(own - after - jnp.concatenate([carry] * (bk // 128), axis=1))
        if masked:
            a = jnp.where(keep, a, 0.0)
        acc_ref[acc0 : acc0 + nrows, :] += jnp.dot(
            a.astype(bf), v_ref[pl.ds(col0, bk), :], preferred_element_type=jnp.float32
        )
        car_ref[acc0 : acc0 + nrows, :] = carry + jnp.broadcast_to((after + soft)[:, :1], (nrows, 128))

    per = bq // bk
    quarter = rows // 2

    def q_tile(i, _):
        base = pl.multiple_of(i * bq, bq)
        acc_ref[...] = jnp.zeros_like(acc_ref)
        car_ref[...] = jnp.zeros_like(car_ref)
        for c in reversed(range(per)):
            for r in range(c, per):
                tile(base + r * bk, bk, r * bk, base + c * bk, r == c)

        def k_tile(j, _):
            col = pl.multiple_of((i - 1 - j) * bq, bq)
            for c in reversed(range(per)):
                tile(base, bq, 0, col + c * bk, False)
            return 0

        lax.fori_loop(0, i, k_tile, 0)
        att = acc_ref[...]
        scaled = att * lax.rsqrt(jnp.mean(att * att, axis=1, keepdims=True) + norm_eps) * gain_ref[...]
        head = scaled.astype(bf)
        count = bq // quarter
        for p in range(count // 2):
            out_ref[pl.ds(i * (count // 2) + p, 1)] = jnp.concatenate(
                [head[2 * p * quarter : (2 * p + 1) * quarter], head[(2 * p + 1) * quarter : (2 * p + 2) * quarter]],
                axis=1,
            )[None]
        return 0

    lax.fori_loop(0, length // bq, q_tile, 0)


def output_kernel(got_ref, own_ref, far_ref, out_ref, heads_ref):
    x, c, z, y = place_of()
    half = got_ref.shape[1]
    for iz in range(SIDE):
        for iy in range(SIDE):
            place = SIDE * lax.rem(z + SIDE - HOPS[iz], SIDE) + lax.rem(y + SIDE - HOPS[iy], SIDE)
            block = got_ref[place]
            at = (SIDE * iz + iy) * HEAD_DIM
            heads_ref[:half, at : at + HEAD_DIM] = block[:, :HEAD_DIM]
            heads_ref[half:, at : at + HEAD_DIM] = block[:, HEAD_DIM:]
    for i in range(SIDE):
        for cc, ref in ((0, own_ref), (1, far_ref)):
            parts = []
            for iz in range(SIDE):
                for iy in range(SIDE):
                    parts.append(ref[i, iz, iy])
            mixed = jnp.dot(
                heads_ref[...], jnp.concatenate(parts, axis=0), preferred_element_type=jnp.float32
            )
            chunk = 2 * lax.rem(x + SIDE - HOPS[i], SIDE) + lax.rem(c + cc, 2)
            out_ref[:, pl.ds(pl.multiple_of(chunk * 256, 256), 256)] = mixed.astype(jnp.bfloat16)


def body(inputs, in_gain, w_query, w_key, w_value, key_bias, out_gain, w_out):
    bf = jnp.bfloat16
    rows, width = inputs.shape[1], inputs.shape[2]
    sp_size = lax.axis_size("sp")
    sp = lax.axis_index("sp")

    wide = inputs[0].astype(jnp.float32)
    normed = (
        wide * lax.rsqrt(jnp.mean(wide * wide, axis=-1, keepdims=True) + norm_eps) * in_gain
    ).astype(bf)

    def spread(perm_of, a, axis):
        return [a] + [lax.ppermute(a, axis, perm_of(k)) for k in HOPS[1:]]

    piece = jnp.concatenate([w_query.T, w_key.T, w_value.T], axis=0)
    four = jnp.stack(spread(along_x, piece, "dp"))
    rest_y = jnp.stack(spread(lambda k: along_zy(0, k), w_out, "sp"))
    first_a = jnp.stack(spread(lambda k: along_zy(0, k), four[:2], "sp"))
    together = jnp.concatenate([four[2:].reshape(192, 256), rest_y.reshape(256, 256)], axis=0)
    first_b = jnp.stack(spread(lambda k: along_zy(k, 0), together, "sp"))
    rest_z = first_b[:, 192:].reshape(SIDE, SIDE, 64, 256)
    first_b = first_b[:, :192].reshape(SIDE, 2, 96, 256)
    first_a, first_b, normed = lax.optimization_barrier((first_a, first_b, normed))
    own_a = spread(lambda k: along_zy(k, 0), first_a, "sp")
    own_b = spread(lambda k: along_zy(0, k), first_b, "sp")
    own_a, own_b = jnp.stack(own_a), jnp.stack(own_b)
    far_a = lax.ppermute(own_a, "dp", other_core())
    far_b = lax.ppermute(own_b, "dp", other_core())
    packed = pl.pallas_call(
        project_kernel,
        out_shape=pltpu.VMEM((sp_size, rows + rows // 2, 128), bf),
        in_specs=[VMEM] * 5,
        out_specs=VMEM,
        scratch_shapes=[pltpu.VMEM((rows, width), bf), pltpu.VMEM((sp_size, 96, rows), jnp.float32)],
        compiler_params=pltpu.CompilerParams(vmem_limit_bytes=30 * 2**20),
        name="project",
    )(*near(normed, own_a, own_b, far_a, far_b))
    packed, rest_z = lax.optimization_barrier((packed, rest_z))
    rest_x = spread(along_x, rest_z, "dp")

    got = lax.all_to_all(packed, "sp", split_axis=0, concat_axis=0, tiled=True)
    gains = lax.dynamic_slice_in_dim(out_gain, sp * HEAD_DIM, HEAD_DIM, 0)[None]
    length = sp_size * rows
    bq, bk = 768, 256
    heads = pl.pallas_call(
        functools.partial(attend_kernel, src=sp_size, rows=rows, bq=bq, bk=bk),
        out_shape=pltpu.VMEM((sp_size, rows // 2, 128), bf),
        in_specs=[VMEM] * 3,
        out_specs=VMEM,
        scratch_shapes=[
            pltpu.VMEM((length, 256), bf),
            pltpu.VMEM((256, length), bf),
            pltpu.VMEM((length, HEAD_DIM), bf),
            pltpu.VMEM((bq, HEAD_DIM), jnp.float32),
            pltpu.VMEM((bq, 128), jnp.float32),
        ],
        compiler_params=pltpu.CompilerParams(vmem_limit_bytes=30 * 2**20),
        name="attend",
    )(*near(got, key_bias.reshape(1, length), gains))
    heads, rest_x = lax.optimization_barrier((heads, rest_x))
    own_out = jnp.stack(rest_x)
    far_out = lax.ppermute(own_out, "dp", other_core())
    returned = lax.all_to_all(heads, "sp", split_axis=0, concat_axis=0, tiled=True)
    mixed = pl.pallas_call(
        output_kernel,
        out_shape=jax.ShapeDtypeStruct((rows, width), bf),
        in_specs=[VMEM] * 3,
        out_specs=VMEM,
        scratch_shapes=[pltpu.VMEM((rows, sp_size * HEAD_DIM), bf)],
        compiler_params=pltpu.CompilerParams(vmem_limit_bytes=30 * 2**20),
        name="output",
    )(*near(returned, own_out, far_out))
    return mixed[None]


def solution(mesh):
    placed = (
        P("dp", "sp", None),
        P(),
        P("dp", "sp"),
        P("dp", "sp"),
        P("dp", "sp"),
        P("dp", None, "sp"),
        P(),
        P("sp", "dp"),
    )
    return jax.shard_map(
        body, mesh=mesh, in_specs=placed, out_specs=P("dp", "sp", None), check_vma=False
    )
```

```python
import functools
import math

import jax
import jax.numpy as jnp
from jax import lax
from jax.experimental import pallas as pl
from jax.experimental.pallas import tpu as pltpu
from jax.sharding import PartitionSpec as P

HEAD_DIM = 64
LOG2E = math.log2(math.e)
norm_eps = 1e-06
SIDE = 4
HOPS = (0, 1, 3, 2)


VMEM = pl.BlockSpec(memory_space=pltpu.VMEM)


def along_x(k):
    return [(i, (i + 2 * k) % (2 * SIDE)) for i in range(2 * SIDE)]


def other_core():
    return [(i, i ^ 1) for i in range(2 * SIDE)]


def along_zy(dz, dy):
    return [
        (s, ((s // SIDE + dz) % SIDE) * SIDE + (s % SIDE + dy) % SIDE) for s in range(SIDE * SIDE)
    ]


def near(*arrays):
    return [pltpu.with_memory_space_constraint(a, pltpu.VMEM) for a in arrays]


def place_of():
    dp, sp = lax.axis_index("dp"), lax.axis_index("sp")
    return lax.div(dp, 2), lax.rem(dp, 2), lax.div(sp, SIDE), lax.rem(sp, SIDE)


def project_kernel(normed_ref, own_a, own_b, far_a, far_b, out_ref, order_ref, sums_ref):
    bf = jnp.bfloat16
    x, c, z, y = place_of()
    rows = normed_ref.shape[0]
    for i in range(SIDE):
        for cc in range(2):
            chunk = 2 * lax.rem(x + SIDE - HOPS[i], SIDE) + lax.rem(c + cc, 2)
            order_ref[:, (2 * i + cc) * 256 : (2 * i + cc + 1) * 256] = normed_ref[
                :, pl.ds(pl.multiple_of(chunk * 256, 256), 256)
            ]
    for iz in range(SIDE):
        parts = []
        for i in range(SIDE):
            for ref_a, ref_b in ((own_a, own_b), (far_a, far_b)):
                if i < 2:
                    parts.append(jnp.concatenate([ref_a[iz, iy, i] for iy in range(SIDE)], axis=0))
                else:
                    parts.append(jnp.concatenate([ref_b[iy, iz, i - 2] for iy in range(SIDE)], axis=0))
        weights = jnp.concatenate(parts, axis=1)
        total = lax.dot_general(
            weights, order_ref[...], (((1,), (1,)), ((), ())), preferred_element_type=jnp.float32
        )
        for iy in range(SIDE):
            place = SIDE * lax.rem(z + SIDE - HOPS[iz], SIDE) + lax.rem(y + SIDE - HOPS[iy], SIDE)
            sums_ref[place] = total[96 * iy : 96 * (iy + 1), :]
    half = rows // 2
    for g in range(SIDE):
        key = jnp.concatenate([sums_ref[SIDE * g + j, 64:80, :] for j in range(SIDE)], axis=0)
        value = jnp.concatenate([sums_ref[SIDE * g + j, 80:96, :] for j in range(SIDE)], axis=0)
        turned = value.T.astype(bf)
        for j in range(SIDE):
            h = SIDE * g + j
            both = jnp.concatenate([sums_ref[h, :64, :], key], axis=0)
            out_ref[h, :rows, :] = both.T.astype(bf)
            out_ref[h, rows:, :] = jnp.concatenate([turned[:half], turned[half:]], axis=1)


def attend_kernel(got_ref, bias_ref, gain_ref, out_ref, qa_ref, kt_ref, v_ref, acc_ref, car_ref, *, src, rows, bq, bk):
    bf = jnp.bfloat16
    half = rows // 2
    length = src * rows
    lane = lax.broadcasted_iota(jnp.int32, (rows, 128), 1)
    ones = jnp.where(lane < 3, 1.0, 0.0).astype(bf)
    for b in range(src):
        both = got_ref[b, :rows, :]
        wide = both[:, :HEAD_DIM].astype(jnp.float32) * (LOG2E * HEAD_DIM ** -0.5)
        high = wide.astype(bf)
        low = (wide - high.astype(jnp.float32)).astype(bf)
        qa_ref[b * rows : (b + 1) * rows, :128] = jnp.concatenate([high, low], axis=1)
        qa_ref[b * rows : (b + 1) * rows, 128:] = ones
        vv = got_ref[b, rows:, :]
        v_ref[b * rows : b * rows + half, :] = vv[:, :HEAD_DIM]
        v_ref[b * rows + half : (b + 1) * rows, :] = vv[:, HEAD_DIM:]
    step = 2 * rows
    for b in range(src // 2):
        pair = jnp.concatenate([got_ref[2 * b, :rows, :], got_ref[2 * b + 1, :rows, :]], axis=0)
        kt = pair.astype(jnp.float32).T[HEAD_DIM:, :].astype(bf)
        kt_ref[:HEAD_DIM, b * step : (b + 1) * step] = kt
        kt_ref[HEAD_DIM : 2 * HEAD_DIM, b * step : (b + 1) * step] = kt
    b2 = bias_ref[...] * LOG2E
    b_high = b2.astype(bf).astype(jnp.float32)
    b_mid = (b2 - b_high).astype(bf).astype(jnp.float32)
    b_low = b2 - b_high - b_mid
    row = lax.broadcasted_iota(jnp.int32, (128, length), 0)
    tail = jnp.where(row == 0, b_high, jnp.where(row == 1, b_mid, jnp.where(row == 2, b_low, 0.0)))
    kt_ref[2 * HEAD_DIM :, :] = tail.astype(bf)

    tri = (
        lax.broadcasted_iota(jnp.int32, (bk, bk), 0) > lax.broadcasted_iota(jnp.int32, (bk, bk), 1)
    ).astype(bf)

    def tile(row0, nrows, acc0, col0, masked):
        x = jnp.dot(
            qa_ref[pl.ds(row0, nrows), :], kt_ref[:, pl.ds(col0, bk)], preferred_element_type=jnp.float32
        )
        soft = jnp.maximum(x, jnp.log2(1.0 + jnp.exp2(jnp.minimum(x, 126.0))))
        own = x - soft
        if masked:
            keep = lax.broadcasted_iota(jnp.int32, (nrows, bk), 1) < lax.broadcasted_iota(
                jnp.int32, (nrows, bk), 0
            )
            soft = jnp.where(keep, soft, 0.0)
        after = jnp.dot(soft.astype(bf), tri, preferred_element_type=jnp.float32)
        carry = car_ref[acc0 : acc0 + nrows, :]
        a = jnp.exp2(own - after - jnp.concatenate([carry] * (bk // 128), axis=1))
        if masked:
            a = jnp.where(keep, a, 0.0)
        acc_ref[acc0 : acc0 + nrows, :] += jnp.dot(
            a.astype(bf), v_ref[pl.ds(col0, bk), :], preferred_element_type=jnp.float32
        )
        car_ref[acc0 : acc0 + nrows, :] = carry + jnp.broadcast_to((after + soft)[:, :1], (nrows, 128))

    per = bq // bk
    quarter = rows // 2

    def q_tile(i, _):
        base = pl.multiple_of(i * bq, bq)
        acc_ref[...] = jnp.zeros_like(acc_ref)
        car_ref[...] = jnp.zeros_like(car_ref)
        for c in reversed(range(per)):
            for r in range(c, per):
                tile(base + r * bk, bk, r * bk, base + c * bk, r == c)

        def k_tile(j, _):
            col = pl.multiple_of((i - 1 - j) * bq, bq)
            for c in reversed(range(per)):
                tile(base, bq, 0, col + c * bk, False)
            return 0

        lax.fori_loop(0, i, k_tile, 0)
        att = acc_ref[...]
        scaled = att * lax.rsqrt(jnp.mean(att * att, axis=1, keepdims=True) + norm_eps) * gain_ref[...]
        head = scaled.astype(bf)
        count = bq // quarter
        for p in range(count // 2):
            out_ref[pl.ds(i * (count // 2) + p, 1)] = jnp.concatenate(
                [head[2 * p * quarter : (2 * p + 1) * quarter], head[(2 * p + 1) * quarter : (2 * p + 2) * quarter]],
                axis=1,
            )[None]
        return 0

    lax.fori_loop(0, length // bq, q_tile, 0)


def output_kernel(got_ref, own_ref, far_ref, out_ref, heads_ref):
    x, c, z, y = place_of()
    half = got_ref.shape[1]
    for iz in range(SIDE):
        for iy in range(SIDE):
            place = SIDE * lax.rem(z + SIDE - HOPS[iz], SIDE) + lax.rem(y + SIDE - HOPS[iy], SIDE)
            block = got_ref[place]
            at = (SIDE * iz + iy) * HEAD_DIM
            heads_ref[:half, at : at + HEAD_DIM] = block[:, :HEAD_DIM]
            heads_ref[half:, at : at + HEAD_DIM] = block[:, HEAD_DIM:]
    for i in range(SIDE):
        for cc, ref in ((0, own_ref), (1, far_ref)):
            parts = []
            for iz in range(SIDE):
                for iy in range(SIDE):
                    parts.append(ref[i, iz, iy])
            mixed = jnp.dot(
                heads_ref[...], jnp.concatenate(parts, axis=0), preferred_element_type=jnp.float32
            )
            chunk = 2 * lax.rem(x + SIDE - HOPS[i], SIDE) + lax.rem(c + cc, 2)
            out_ref[:, pl.ds(pl.multiple_of(chunk * 256, 256), 256)] = mixed.astype(jnp.bfloat16)


def body(inputs, in_gain, w_query, w_key, w_value, key_bias, out_gain, w_out):
    bf = jnp.bfloat16
    rows, width = inputs.shape[1], inputs.shape[2]
    sp_size = lax.axis_size("sp")
    sp = lax.axis_index("sp")

    wide = inputs[0].astype(jnp.float32)
    normed = (
        wide * lax.rsqrt(jnp.mean(wide * wide, axis=-1, keepdims=True) + norm_eps) * in_gain
    ).astype(bf)

    def spread(perm_of, a, axis):
        return [a] + [lax.ppermute(a, axis, perm_of(k)) for k in HOPS[1:]]

    piece = jnp.concatenate([w_query.T, w_key.T, w_value.T], axis=0)
    four = jnp.stack(spread(along_x, piece, "dp"))
    together = jnp.concatenate([four[:2].reshape(192, 256), w_out], axis=0)
    first_a = jnp.stack(spread(lambda k: along_zy(0, k), together, "sp"))
    first_b = jnp.stack(spread(lambda k: along_zy(k, 0), four[2:], "sp"))
    rest_y = first_a[:, 192:]
    first_a = first_a[:, :192].reshape(SIDE, 2, 96, 256)
    first_a, first_b, normed = lax.optimization_barrier((first_a, first_b, normed))
    own_a = spread(lambda k: along_zy(k, 0), first_a, "sp")
    own_b = spread(lambda k: along_zy(0, k), first_b, "sp")
    own_a, own_b = jnp.stack(own_a), jnp.stack(own_b)
    own_a, rest_y = lax.optimization_barrier((own_a, rest_y))
    far_a = lax.ppermute(own_a, "dp", other_core())
    far_b = lax.ppermute(own_b, "dp", other_core())
    packed = pl.pallas_call(
        project_kernel,
        out_shape=pltpu.VMEM((sp_size, rows + rows // 2, 128), bf),
        in_specs=[VMEM] * 5,
        out_specs=VMEM,
        scratch_shapes=[pltpu.VMEM((rows, width), bf), pltpu.VMEM((sp_size, 96, rows), jnp.float32)],
        compiler_params=pltpu.CompilerParams(vmem_limit_bytes=30 * 2**20),
        name="project",
    )(*near(normed, own_a, own_b, far_a, far_b))
    rest_z = spread(lambda k: along_zy(k, 0), rest_y, "sp")
    _, rest_z = lax.optimization_barrier((packed, rest_z))
    rest_x = spread(along_x, jnp.stack(rest_z), "dp")

    got = lax.all_to_all(packed, "sp", split_axis=0, concat_axis=0, tiled=True)
    gains = lax.dynamic_slice_in_dim(out_gain, sp * HEAD_DIM, HEAD_DIM, 0)[None]
    length = sp_size * rows
    bq, bk = 768, 256
    heads = pl.pallas_call(
        functools.partial(attend_kernel, src=sp_size, rows=rows, bq=bq, bk=bk),
        out_shape=pltpu.VMEM((sp_size, rows // 2, 128), bf),
        in_specs=[VMEM] * 3,
        out_specs=VMEM,
        scratch_shapes=[
            pltpu.VMEM((length, 256), bf),
            pltpu.VMEM((256, length), bf),
            pltpu.VMEM((length, HEAD_DIM), bf),
            pltpu.VMEM((bq, HEAD_DIM), jnp.float32),
            pltpu.VMEM((bq, 128), jnp.float32),
        ],
        compiler_params=pltpu.CompilerParams(vmem_limit_bytes=30 * 2**20),
        name="attend",
    )(*near(got, key_bias.reshape(1, length), gains))
    heads, rest_x = lax.optimization_barrier((heads, rest_x))
    own_out = jnp.stack(rest_x)
    far_out = lax.ppermute(own_out, "dp", other_core())
    returned = lax.all_to_all(heads, "sp", split_axis=0, concat_axis=0, tiled=True)
    mixed = pl.pallas_call(
        output_kernel,
        out_shape=jax.ShapeDtypeStruct((rows, width), bf),
        in_specs=[VMEM] * 3,
        out_specs=VMEM,
        scratch_shapes=[pltpu.VMEM((rows, sp_size * HEAD_DIM), bf)],
        compiler_params=pltpu.CompilerParams(vmem_limit_bytes=30 * 2**20),
        name="output",
    )(*near(returned, own_out, far_out))
    return mixed[None]


def solution(mesh):
    placed = (
        P("dp", "sp", None),
        P(),
        P("dp", "sp"),
        P("dp", "sp"),
        P("dp", "sp"),
        P("dp", None, "sp"),
        P(),
        P("sp", "dp"),
    )

    return jax.shard_map(body, mesh=mesh, in_specs=placed, out_specs=P("dp", "sp", None), check_vma=False)
```

```python
import functools
import math

import jax
import jax.numpy as jnp
from jax import lax
from jax.experimental import pallas as pl
from jax.experimental.pallas import tpu as pltpu
from jax.sharding import PartitionSpec as P

HEAD_DIM = 64
LOG2E = math.log2(math.e)
norm_eps = 1e-06
SIDE = 4
HOPS = (0, 1, 3, 2)


VMEM = pl.BlockSpec(memory_space=pltpu.VMEM)


def along_x(k):
    return [(i, (i + 2 * k) % (2 * SIDE)) for i in range(2 * SIDE)]


def other_core():
    return [(i, i ^ 1) for i in range(2 * SIDE)]


def along_zy(dz, dy):
    return [
        (s, ((s // SIDE + dz) % SIDE) * SIDE + (s % SIDE + dy) % SIDE) for s in range(SIDE * SIDE)
    ]


def near(*arrays):
    return [pltpu.with_memory_space_constraint(a, pltpu.VMEM) for a in arrays]


def place_of():
    dp, sp = lax.axis_index("dp"), lax.axis_index("sp")
    return lax.div(dp, 2), lax.rem(dp, 2), lax.div(sp, SIDE), lax.rem(sp, SIDE)


def project_kernel(normed_ref, own_a, own_b, far_a, far_b, out_ref, order_ref, sums_ref):
    bf = jnp.bfloat16
    x, c, z, y = place_of()
    rows = normed_ref.shape[0]
    for i in range(SIDE):
        for cc in range(2):
            chunk = 2 * lax.rem(x + SIDE - HOPS[i], SIDE) + lax.rem(c + cc, 2)
            order_ref[:, (2 * i + cc) * 256 : (2 * i + cc + 1) * 256] = normed_ref[
                :, pl.ds(pl.multiple_of(chunk * 256, 256), 256)
            ]
    for iz in range(SIDE):
        parts = []
        for i in range(SIDE):
            for ref_a, ref_b in ((own_a, own_b), (far_a, far_b)):
                if i < 2:
                    parts.append(jnp.concatenate([ref_a[iz, iy, i] for iy in range(SIDE)], axis=0))
                else:
                    parts.append(jnp.concatenate([ref_b[iy, iz, i - 2] for iy in range(SIDE)], axis=0))
        weights = jnp.concatenate(parts, axis=1)
        total = lax.dot_general(
            weights, order_ref[...], (((1,), (1,)), ((), ())), preferred_element_type=jnp.float32
        )
        for iy in range(SIDE):
            place = SIDE * lax.rem(z + SIDE - HOPS[iz], SIDE) + lax.rem(y + SIDE - HOPS[iy], SIDE)
            sums_ref[place] = total[96 * iy : 96 * (iy + 1), :]
    half = rows // 2
    for g in range(SIDE):
        key = jnp.concatenate([sums_ref[SIDE * g + j, 64:80, :] for j in range(SIDE)], axis=0)
        value = jnp.concatenate([sums_ref[SIDE * g + j, 80:96, :] for j in range(SIDE)], axis=0)
        turned = value.T.astype(bf)
        for j in range(SIDE):
            h = SIDE * g + j
            both = jnp.concatenate([sums_ref[h, :64, :], key], axis=0)
            out_ref[h, :rows, :] = both.T.astype(bf)
            out_ref[h, rows:, :] = jnp.concatenate([turned[:half], turned[half:]], axis=1)


def masked(block, mask):
    rows = mask.shape[0]
    first = block[:rows] * mask
    return first if block.shape[0] == rows else jnp.concatenate([first, block[rows:]], axis=0)


def attend_kernel(
    got_ref, bias_ref, gain_ref, out_ref, qa_ref, kt_ref, v_ref, acc_ref, car_ref, mask_ref, tri_ref, *, src, rows, bk
):
    bf = jnp.bfloat16
    half = rows // 2
    length = src * rows
    lane = lax.broadcasted_iota(jnp.int32, (rows, 128), 1)
    ones = jnp.where(lane < 3, 1.0, 0.0).astype(bf)
    for b in range(src):
        both = got_ref[b, :rows, :]
        wide = both[:, :HEAD_DIM].astype(jnp.float32) * (LOG2E * HEAD_DIM ** -0.5)
        high = wide.astype(bf)
        low = (wide - high.astype(jnp.float32)).astype(bf)
        qa_ref[b * rows : (b + 1) * rows, :128] = jnp.concatenate([high, low], axis=1)
        qa_ref[b * rows : (b + 1) * rows, 128:] = ones
        vv = got_ref[b, rows:, :]
        v_ref[b * rows : b * rows + half, :] = vv[:, :HEAD_DIM]
        v_ref[b * rows + half : (b + 1) * rows, :] = vv[:, HEAD_DIM:]
    step = 2 * rows
    for b in range(src // 2):
        pair = jnp.concatenate([got_ref[2 * b, :rows, :], got_ref[2 * b + 1, :rows, :]], axis=0)
        kt = pair.astype(jnp.float32).T[HEAD_DIM:, :].astype(bf)
        kt_ref[:HEAD_DIM, b * step : (b + 1) * step] = kt
        kt_ref[HEAD_DIM : 2 * HEAD_DIM, b * step : (b + 1) * step] = kt
    b2 = bias_ref[...] * LOG2E
    b_high = b2.astype(bf).astype(jnp.float32)
    b_mid = (b2 - b_high).astype(bf).astype(jnp.float32)
    b_low = b2 - b_high - b_mid
    row = lax.broadcasted_iota(jnp.int32, (128, length), 0)
    tail = jnp.where(row == 0, b_high, jnp.where(row == 1, b_mid, jnp.where(row == 2, b_low, 0.0)))
    kt_ref[2 * HEAD_DIM :, :] = tail.astype(bf)

    below = lax.broadcasted_iota(jnp.int32, (bk, bk), 0) > lax.broadcasted_iota(jnp.int32, (bk, bk), 1)
    mask_ref[...] = jnp.where(below, 1.0, 0.0)
    tri_ref[...] = jnp.where(below, 1.0, 0.0).astype(bf)
    acc_ref[...] = jnp.zeros_like(acc_ref)
    car_ref[...] = jnp.zeros_like(car_ref)

    for c in reversed(range(length // bk)):
        at = c * bk
        x = jnp.dot(qa_ref[at:, :], kt_ref[:, at : at + bk], preferred_element_type=jnp.float32)
        soft = jnp.maximum(x, jnp.log2(1.0 + jnp.exp2(jnp.minimum(x, 126.0))))
        own = x - soft
        soft = masked(soft, mask_ref[...])
        after = jnp.dot(soft.astype(bf), tri_ref[...], preferred_element_type=jnp.float32)
        a = masked(jnp.exp2(own - after), mask_ref[...])
        carry = car_ref[at:, :]
        here = jnp.dot(a.astype(bf), v_ref[at : at + bk, :], preferred_element_type=jnp.float32)
        acc_ref[at:, :] += here * jnp.exp2(-carry)[:, :HEAD_DIM]
        total = after[:, :128] + soft[:, :128]
        car_ref[at:, :] = carry + jnp.broadcast_to(total[:, :1], carry.shape)

    for b in range(src):
        att = acc_ref[b * rows : (b + 1) * rows, :]
        scaled = att * lax.rsqrt(jnp.mean(att * att, axis=1, keepdims=True) + norm_eps) * gain_ref[...]
        head = scaled.astype(bf)
        out_ref[b] = jnp.concatenate([head[:half], head[half:]], axis=1)


def output_kernel(got_ref, own_ref, far_ref, out_ref, heads_ref):
    x, c, z, y = place_of()
    half = got_ref.shape[1]
    for iz in range(SIDE):
        for iy in range(SIDE):
            place = SIDE * lax.rem(z + SIDE - HOPS[iz], SIDE) + lax.rem(y + SIDE - HOPS[iy], SIDE)
            block = got_ref[place]
            at = (SIDE * iz + iy) * HEAD_DIM
            heads_ref[:half, at : at + HEAD_DIM] = block[:, :HEAD_DIM]
            heads_ref[half:, at : at + HEAD_DIM] = block[:, HEAD_DIM:]
    for i in range(SIDE):
        for cc, ref in ((0, own_ref), (1, far_ref)):
            parts = []
            for iz in range(SIDE):
                for iy in range(SIDE):
                    parts.append(ref[i, iz, iy])
            mixed = jnp.dot(
                heads_ref[...], jnp.concatenate(parts, axis=0), preferred_element_type=jnp.float32
            )
            chunk = 2 * lax.rem(x + SIDE - HOPS[i], SIDE) + lax.rem(c + cc, 2)
            out_ref[:, pl.ds(pl.multiple_of(chunk * 256, 256), 256)] = mixed.astype(jnp.bfloat16)


def body(inputs, in_gain, w_query, w_key, w_value, key_bias, out_gain, w_out):
    bf = jnp.bfloat16
    rows, width = inputs.shape[1], inputs.shape[2]
    sp_size = lax.axis_size("sp")
    sp = lax.axis_index("sp")

    wide = inputs[0].astype(jnp.float32)
    normed = (
        wide * lax.rsqrt(jnp.mean(wide * wide, axis=-1, keepdims=True) + norm_eps) * in_gain
    ).astype(bf)

    def spread(perm_of, a, axis):
        return [a] + [lax.ppermute(a, axis, perm_of(k)) for k in HOPS[1:]]

    piece = jnp.concatenate([w_query.T, w_key.T, w_value.T], axis=0)
    four = jnp.stack(spread(along_x, piece, "dp"))
    together = jnp.concatenate([four[:2].reshape(192, 256), w_out], axis=0)
    first_a = jnp.stack(spread(lambda k: along_zy(0, k), together, "sp"))
    first_b = jnp.stack(spread(lambda k: along_zy(k, 0), four[2:], "sp"))
    rest_y = first_a[:, 192:]
    first_a = first_a[:, :192].reshape(SIDE, 2, 96, 256)
    first_a, first_b, normed = lax.optimization_barrier((first_a, first_b, normed))
    own_a = spread(lambda k: along_zy(k, 0), first_a, "sp")
    own_b = spread(lambda k: along_zy(0, k), first_b, "sp")
    own_a, own_b = jnp.stack(own_a), jnp.stack(own_b)
    own_a, rest_y = lax.optimization_barrier((own_a, rest_y))
    far_a = lax.ppermute(own_a, "dp", other_core())
    far_b = lax.ppermute(own_b, "dp", other_core())
    packed = pl.pallas_call(
        project_kernel,
        out_shape=pltpu.VMEM((sp_size, rows + rows // 2, 128), bf),
        in_specs=[VMEM] * 5,
        out_specs=VMEM,
        scratch_shapes=[pltpu.VMEM((rows, width), bf), pltpu.VMEM((sp_size, 96, rows), jnp.float32)],
        compiler_params=pltpu.CompilerParams(vmem_limit_bytes=30 * 2**20),
        name="project",
    )(*near(normed, own_a, own_b, far_a, far_b))
    rest_z = spread(lambda k: along_zy(k, 0), rest_y, "sp")
    _, rest_z = lax.optimization_barrier((packed, rest_z))
    rest_x = spread(along_x, jnp.stack(rest_z), "dp")

    got = lax.all_to_all(packed, "sp", split_axis=0, concat_axis=0, tiled=True)
    gains = lax.dynamic_slice_in_dim(out_gain, sp * HEAD_DIM, HEAD_DIM, 0)[None]
    length = sp_size * rows
    bk = 256
    heads = pl.pallas_call(
        functools.partial(attend_kernel, src=sp_size, rows=rows, bk=bk),
        out_shape=pltpu.VMEM((sp_size, rows // 2, 128), bf),
        in_specs=[VMEM] * 3,
        out_specs=VMEM,
        scratch_shapes=[
            pltpu.VMEM((length, 256), bf),
            pltpu.VMEM((256, length), bf),
            pltpu.VMEM((length, HEAD_DIM), bf),
            pltpu.VMEM((length, HEAD_DIM), jnp.float32),
            pltpu.VMEM((length, 128), jnp.float32),
            pltpu.VMEM((bk, bk), jnp.float32),
            pltpu.VMEM((bk, bk), bf),
        ],
        compiler_params=pltpu.CompilerParams(vmem_limit_bytes=30 * 2**20),
        name="attend",
    )(*near(got, key_bias.reshape(1, length), gains))
    heads, rest_x = lax.optimization_barrier((heads, rest_x))
    own_out = jnp.stack(rest_x)
    far_out = lax.ppermute(own_out, "dp", other_core())
    returned = lax.all_to_all(heads, "sp", split_axis=0, concat_axis=0, tiled=True)
    mixed = pl.pallas_call(
        output_kernel,
        out_shape=jax.ShapeDtypeStruct((rows, width), bf),
        in_specs=[VMEM] * 3,
        out_specs=VMEM,
        scratch_shapes=[pltpu.VMEM((rows, sp_size * HEAD_DIM), bf)],
        compiler_params=pltpu.CompilerParams(vmem_limit_bytes=30 * 2**20),
        name="output",
    )(*near(returned, own_out, far_out))
    return mixed[None]


def solution(mesh):
    placed = (
        P("dp", "sp", None),
        P(),
        P("dp", "sp"),
        P("dp", "sp"),
        P("dp", "sp"),
        P("dp", None, "sp"),
        P(),
        P("sp", "dp"),
    )

    return jax.shard_map(body, mesh=mesh, in_specs=placed, out_specs=P("dp", "sp", None), check_vma=False)
```

```python
import functools
import math

import jax
import jax.numpy as jnp
from jax import lax
from jax.experimental import pallas as pl
from jax.experimental.pallas import tpu as pltpu
from jax.sharding import PartitionSpec as P

HEAD_DIM = 64
LOG2E = math.log2(math.e)
norm_eps = 1e-06
SIDE = 4


VMEM = pl.BlockSpec(memory_space=pltpu.VMEM)


def pairs(step, size):
    return [(i, i ^ step) for i in range(size)]


def along_x(k):
    return [(i, (i + 2 * k) % (2 * SIDE)) for i in range(2 * SIDE)]


def along_zy(dz, dy):
    return [
        (s, ((s // SIDE + dz) % SIDE) * SIDE + (s % SIDE + dy) % SIDE) for s in range(SIDE * SIDE)
    ]


def doubled(a, axis, perms):
    for perm in perms:
        a = jnp.concatenate([a, lax.ppermute(a, axis, perm)], axis=0)
    return a


def both_ways(a, axis, perm_of):
    back = lax.ppermute(a, axis, perm_of(1))
    ahead = lax.ppermute(a, axis, perm_of(-1))
    half = a.shape[0] // 2
    low = lax.ppermute(back[:half], axis, perm_of(1))
    high = lax.ppermute(ahead[half:], axis, perm_of(-1))
    return jnp.stack([a, back, jnp.concatenate([low, high], axis=0), ahead])


def near(*arrays):
    return [pltpu.with_memory_space_constraint(a, pltpu.VMEM) for a in arrays]


def place_of():
    dp, sp = lax.axis_index("dp"), lax.axis_index("sp")
    return lax.div(dp, 2), lax.rem(dp, 2), lax.div(sp, SIDE), lax.rem(sp, SIDE)


def before(here, there):
    return lax.rem(here + SIDE - there, SIDE)


def project_kernel(normed_ref, own_a, own_b, far_a, far_b, out_ref, done_ref, order_ref, sums_ref):
    bf = jnp.bfloat16
    x, c, z, y = place_of()
    rows = normed_ref.shape[0]
    for i in range(SIDE):
        for cc in range(2):
            chunk = 2 * jnp.bitwise_xor(x, i) + jnp.bitwise_xor(c, cc)
            order_ref[:, (2 * i + cc) * 256 : (2 * i + cc + 1) * 256] = normed_ref[
                :, pl.ds(pl.multiple_of(chunk * 256, 256), 256)
            ]
    for zs in range(SIDE):
        parts = []
        for i in range(SIDE):
            for ref_a, ref_b in ((own_a, own_b), (far_a, far_b)):
                if i < 2:
                    several = [ref_a[before(z, zs), jnp.bitwise_xor(y, ys), i] for ys in range(SIDE)]
                else:
                    several = [ref_b[before(y, ys), jnp.bitwise_xor(z, zs), i - 2] for ys in range(SIDE)]
                parts.append(jnp.concatenate(several, axis=0))
        weights = jnp.concatenate(parts, axis=1)
        total = lax.dot_general(
            weights, order_ref[...], (((1,), (1,)), ((), ())), preferred_element_type=jnp.float32
        )
        for ys in range(SIDE):
            sums_ref[SIDE * zs + ys] = total[96 * ys : 96 * (ys + 1), :]
    half = rows // 2
    for g in range(SIDE):
        key = jnp.concatenate([sums_ref[SIDE * g + j, 64:80, :] for j in range(SIDE)], axis=0)
        value = jnp.concatenate([sums_ref[SIDE * g + j, 80:96, :] for j in range(SIDE)], axis=0)
        turned = value.T.astype(bf)
        for j in range(SIDE):
            h = SIDE * g + j
            both = jnp.concatenate([sums_ref[h, :64, :], key], axis=0)
            out_ref[h, :rows, :] = both.T.astype(bf)
            out_ref[h, rows:, :] = jnp.concatenate([turned[:half], turned[half:]], axis=1)
    done_ref[...] = jnp.zeros_like(done_ref)


def masked(block, mask):
    rows = mask.shape[0]
    first = block[:rows] * mask
    return first if block.shape[0] == rows else jnp.concatenate([first, block[rows:]], axis=0)


def attend_kernel(
    got_ref, bias_ref, gain_ref, out_ref, qa_ref, kt_ref, v_ref, acc_ref, car_ref, mask_ref, tri_ref, *, src, rows, bk
):
    bf = jnp.bfloat16
    half = rows // 2
    length = src * rows
    lane = lax.broadcasted_iota(jnp.int32, (rows, 128), 1)
    ones = jnp.where(lane < 3, 1.0, 0.0).astype(bf)
    for b in range(src):
        both = got_ref[b, :rows, :]
        wide = both[:, :HEAD_DIM].astype(jnp.float32) * (LOG2E * HEAD_DIM ** -0.5)
        high = wide.astype(bf)
        low = (wide - high.astype(jnp.float32)).astype(bf)
        qa_ref[b * rows : (b + 1) * rows, :128] = jnp.concatenate([high, low], axis=1)
        qa_ref[b * rows : (b + 1) * rows, 128:] = ones
        vv = got_ref[b, rows:, :]
        v_ref[b * rows : b * rows + half, :] = vv[:, :HEAD_DIM]
        v_ref[b * rows + half : (b + 1) * rows, :] = vv[:, HEAD_DIM:]
    step = 2 * rows
    for b in range(src // 2):
        pair = jnp.concatenate([got_ref[2 * b, :rows, :], got_ref[2 * b + 1, :rows, :]], axis=0)
        kt = pair.astype(jnp.float32).T[HEAD_DIM:, :].astype(bf)
        kt_ref[:HEAD_DIM, b * step : (b + 1) * step] = kt
        kt_ref[HEAD_DIM : 2 * HEAD_DIM, b * step : (b + 1) * step] = kt
    b2 = bias_ref[...] * LOG2E
    b_high = b2.astype(bf).astype(jnp.float32)
    b_mid = (b2 - b_high).astype(bf).astype(jnp.float32)
    b_low = b2 - b_high - b_mid
    row = lax.broadcasted_iota(jnp.int32, (128, length), 0)
    tail = jnp.where(row == 0, b_high, jnp.where(row == 1, b_mid, jnp.where(row == 2, b_low, 0.0)))
    kt_ref[2 * HEAD_DIM :, :] = tail.astype(bf)

    below = lax.broadcasted_iota(jnp.int32, (bk, bk), 0) > lax.broadcasted_iota(jnp.int32, (bk, bk), 1)
    mask_ref[...] = jnp.where(below, 1.0, 0.0)
    tri_ref[...] = jnp.where(below, 1.0, 0.0).astype(bf)
    acc_ref[...] = jnp.zeros_like(acc_ref)
    car_ref[...] = jnp.zeros_like(car_ref)

    for c in reversed(range(length // bk)):
        at = c * bk
        x = jnp.dot(qa_ref[at:, :], kt_ref[:, at : at + bk], preferred_element_type=jnp.float32)
        soft = jnp.maximum(x, jnp.log2(1.0 + jnp.exp2(jnp.minimum(x, 126.0))))
        own = x - soft
        soft = masked(soft, mask_ref[...])
        after = jnp.dot(soft.astype(bf), tri_ref[...], preferred_element_type=jnp.float32)
        a = masked(jnp.exp2(own - after), mask_ref[...])
        carry = car_ref[at:, :]
        here = jnp.dot(a.astype(bf), v_ref[at : at + bk, :], preferred_element_type=jnp.float32)
        acc_ref[at:, :] += here * jnp.exp2(-carry)[:, :HEAD_DIM]
        total = after[:, :128] + soft[:, :128]
        car_ref[at:, :] = carry + jnp.broadcast_to(total[:, :1], carry.shape)

    for b in range(src):
        att = acc_ref[b * rows : (b + 1) * rows, :]
        scaled = att * lax.rsqrt(jnp.mean(att * att, axis=1, keepdims=True) + norm_eps) * gain_ref[...]
        head = scaled.astype(bf)
        out_ref[b] = jnp.concatenate([head[:half], head[half:]], axis=1)


def output_kernel(got_ref, own_ref, far_ref, out_ref, heads_ref):
    x, c, z, y = place_of()
    half = got_ref.shape[1]
    for h in range(SIDE * SIDE):
        block = got_ref[h]
        heads_ref[:half, h * HEAD_DIM : (h + 1) * HEAD_DIM] = block[:, :HEAD_DIM]
        heads_ref[half:, h * HEAD_DIM : (h + 1) * HEAD_DIM] = block[:, HEAD_DIM:]
    for i in range(SIDE):
        for cc, ref in ((0, own_ref), (1, far_ref)):
            parts = [
                ref[i, before(z, zs), jnp.bitwise_xor(y, ys)] for zs in range(SIDE) for ys in range(SIDE)
            ]
            mixed = jnp.dot(
                heads_ref[...], jnp.concatenate(parts, axis=0), preferred_element_type=jnp.float32
            )
            chunk = 2 * before(x, i) + jnp.bitwise_xor(c, cc)
            out_ref[:, pl.ds(pl.multiple_of(chunk * 256, 256), 256)] = mixed.astype(jnp.bfloat16)


def body(inputs, in_gain, w_query, w_key, w_value, key_bias, out_gain, w_out):
    bf = jnp.bfloat16
    rows, width = inputs.shape[1], inputs.shape[2]
    sp_size = lax.axis_size("sp")
    sp = lax.axis_index("sp")

    wide = inputs[0].astype(jnp.float32)
    normed = (
        wide * lax.rsqrt(jnp.mean(wide * wide, axis=-1, keepdims=True) + norm_eps) * in_gain
    ).astype(bf)

    def spread(perm_of, a, axis):
        return [a] + [lax.ppermute(a, axis, perm_of(k)) for k in range(1, SIDE)]

    piece = jnp.concatenate([w_query.T, w_key.T, w_value.T], axis=0)
    four = doubled(piece[None], "dp", (pairs(2, 8), pairs(4, 8)))
    together = jnp.concatenate([four[:2].reshape(192, 256), w_out], axis=0)[None]
    first_a = doubled(together, "sp", (pairs(1, 16), pairs(2, 16)))
    first_b = doubled(four[2:][None], "sp", (pairs(4, 16), pairs(8, 16)))
    rest_y = first_a[:, 192:]
    first_a = first_a[:, :192].reshape(SIDE, 2, 96, 256)
    first_a, first_b, normed = lax.optimization_barrier((first_a, first_b, normed))
    own_a = both_ways(first_a, "sp", lambda k: along_zy(k, 0))
    own_b = both_ways(first_b, "sp", lambda k: along_zy(0, k))
    own_a, rest_y = lax.optimization_barrier((own_a, rest_y))
    far_a = lax.ppermute(own_a, "dp", pairs(1, 8))
    far_b = lax.ppermute(own_b, "dp", pairs(1, 8))
    packed, done = pl.pallas_call(
        project_kernel,
        out_shape=(
            pltpu.VMEM((sp_size, rows + rows // 2, 128), bf),
            jax.ShapeDtypeStruct((8, 128), jnp.float32),
        ),
        in_specs=[VMEM] * 5,
        out_specs=(VMEM, VMEM),
        scratch_shapes=[pltpu.VMEM((rows, width), bf), pltpu.VMEM((sp_size, 96, rows), jnp.float32)],
        compiler_params=pltpu.CompilerParams(vmem_limit_bytes=30 * 2**20),
        name="project",
    )(*near(normed, own_a, own_b, far_a, far_b))
    rest_z = spread(lambda k: along_zy(k, 0), rest_y, "sp")
    _, rest_z = lax.optimization_barrier((done, rest_z))
    rest_x = spread(along_x, jnp.stack(rest_z), "dp")

    got = lax.all_to_all(packed, "sp", split_axis=0, concat_axis=0, tiled=True)
    gains = lax.dynamic_slice_in_dim(out_gain, sp * HEAD_DIM, HEAD_DIM, 0)[None]
    length = sp_size * rows
    bk = 256
    heads = pl.pallas_call(
        functools.partial(attend_kernel, src=sp_size, rows=rows, bk=bk),
        out_shape=pltpu.VMEM((sp_size, rows // 2, 128), bf),
        in_specs=[VMEM] * 3,
        out_specs=VMEM,
        scratch_shapes=[
            pltpu.VMEM((length, 256), bf),
            pltpu.VMEM((256, length), bf),
            pltpu.VMEM((length, HEAD_DIM), bf),
            pltpu.VMEM((length, HEAD_DIM), jnp.float32),
            pltpu.VMEM((length, 128), jnp.float32),
            pltpu.VMEM((bk, bk), jnp.float32),
            pltpu.VMEM((bk, bk), bf),
        ],
        compiler_params=pltpu.CompilerParams(vmem_limit_bytes=30 * 2**20),
        name="attend",
    )(*near(got, key_bias.reshape(1, length), gains))
    heads, rest_x = lax.optimization_barrier((heads, rest_x))
    own_out = jnp.stack(rest_x)
    far_out = lax.ppermute(own_out, "dp", pairs(1, 8))
    returned = lax.all_to_all(heads, "sp", split_axis=0, concat_axis=0, tiled=True)
    mixed = pl.pallas_call(
        output_kernel,
        out_shape=jax.ShapeDtypeStruct((rows, width), bf),
        in_specs=[VMEM] * 3,
        out_specs=VMEM,
        scratch_shapes=[pltpu.VMEM((rows, sp_size * HEAD_DIM), bf)],
        compiler_params=pltpu.CompilerParams(vmem_limit_bytes=30 * 2**20),
        name="output",
    )(*near(returned, own_out, far_out))
    return mixed[None]


def solution(mesh):
    placed = (
        P("dp", "sp", None),
        P(),
        P("dp", "sp"),
        P("dp", "sp"),
        P("dp", "sp"),
        P("dp", None, "sp"),
        P(),
        P("sp", "dp"),
    )

    return jax.shard_map(body, mesh=mesh, in_specs=placed, out_specs=P("dp", "sp", None), check_vma=False)
```

```python
import functools
import math

import jax
import jax.numpy as jnp
from jax import lax
from jax.experimental import pallas as pl
from jax.experimental.pallas import tpu as pltpu
from jax.sharding import PartitionSpec as P

HEAD_DIM = 64
LOG2E = math.log2(math.e)
norm_eps = 1e-06
SIDE = 4


VMEM = pl.BlockSpec(memory_space=pltpu.VMEM)


def pairs(step, size):
    return [(i, i ^ step) for i in range(size)]


def along_x(k):
    return [(i, (i + 2 * k) % (2 * SIDE)) for i in range(2 * SIDE)]


def along_zy(dz, dy):
    return [
        (s, ((s // SIDE + dz) % SIDE) * SIDE + (s % SIDE + dy) % SIDE) for s in range(SIDE * SIDE)
    ]


def doubled(a, axis, perms):
    for perm in perms:
        a = jnp.concatenate([a, lax.ppermute(a, axis, perm)], axis=0)
    return a


def near(*arrays):
    return [pltpu.with_memory_space_constraint(a, pltpu.VMEM) for a in arrays]


def place_of():
    dp, sp = lax.axis_index("dp"), lax.axis_index("sp")
    return lax.div(dp, 2), lax.rem(dp, 2), lax.div(sp, SIDE), lax.rem(sp, SIDE)


def before(here, there):
    return lax.rem(here + SIDE - there, SIDE)


def project_kernel(normed_ref, own_a, own_b, far_a, far_b, out_ref, done_ref, order_ref, sums_ref):
    bf = jnp.bfloat16
    x, c, z, y = place_of()
    rows = normed_ref.shape[0]
    for i in range(SIDE):
        for cc in range(2):
            chunk = 2 * jnp.bitwise_xor(x, i) + jnp.bitwise_xor(c, cc)
            order_ref[:, (2 * i + cc) * 256 : (2 * i + cc + 1) * 256] = normed_ref[
                :, pl.ds(pl.multiple_of(chunk * 256, 256), 256)
            ]
    for zs in range(SIDE):
        parts = []
        for i in range(SIDE):
            for ref_a, ref_b in ((own_a, own_b), (far_a, far_b)):
                if i < 2:
                    several = [ref_a[before(z, zs), jnp.bitwise_xor(y, ys), i] for ys in range(SIDE)]
                else:
                    several = [ref_b[before(y, ys), jnp.bitwise_xor(z, zs), i - 2] for ys in range(SIDE)]
                parts.append(jnp.concatenate(several, axis=0))
        weights = jnp.concatenate(parts, axis=1)
        total = lax.dot_general(
            weights, order_ref[...], (((1,), (1,)), ((), ())), preferred_element_type=jnp.float32
        )
        for ys in range(SIDE):
            sums_ref[SIDE * zs + ys] = total[96 * ys : 96 * (ys + 1), :]
    half = rows // 2
    for g in range(SIDE):
        key = jnp.concatenate([sums_ref[SIDE * g + j, 64:80, :] for j in range(SIDE)], axis=0)
        value = jnp.concatenate([sums_ref[SIDE * g + j, 80:96, :] for j in range(SIDE)], axis=0)
        turned = value.T.astype(bf)
        for j in range(SIDE):
            h = SIDE * g + j
            both = jnp.concatenate([sums_ref[h, :64, :], key], axis=0)
            out_ref[h, :rows, :] = both.T.astype(bf)
            out_ref[h, rows:, :] = jnp.concatenate([turned[:half], turned[half:]], axis=1)
    done_ref[...] = jnp.zeros_like(done_ref)


def masked(block, mask):
    rows = mask.shape[0]
    first = block[:rows] * mask
    return first if block.shape[0] == rows else jnp.concatenate([first, block[rows:]], axis=0)


def attend_kernel(
    got_ref, bias_ref, gain_ref, out_ref, qa_ref, kt_ref, v_ref, acc_ref, car_ref, mask_ref, tri_ref, *, src, rows, bk
):
    bf = jnp.bfloat16
    half = rows // 2
    length = src * rows
    lane = lax.broadcasted_iota(jnp.int32, (rows, 128), 1)
    ones = jnp.where(lane < 3, 1.0, 0.0).astype(bf)
    for b in range(src):
        both = got_ref[b, :rows, :]
        wide = both[:, :HEAD_DIM].astype(jnp.float32) * (LOG2E * HEAD_DIM ** -0.5)
        high = wide.astype(bf)
        low = (wide - high.astype(jnp.float32)).astype(bf)
        qa_ref[b * rows : (b + 1) * rows, :128] = jnp.concatenate([high, low], axis=1)
        qa_ref[b * rows : (b + 1) * rows, 128:] = ones
        vv = got_ref[b, rows:, :]
        v_ref[b * rows : b * rows + half, :] = vv[:, :HEAD_DIM]
        v_ref[b * rows + half : (b + 1) * rows, :] = vv[:, HEAD_DIM:]
    step = 2 * rows
    for b in range(src // 2):
        pair = jnp.concatenate([got_ref[2 * b, :rows, :], got_ref[2 * b + 1, :rows, :]], axis=0)
        kt = pair.astype(jnp.float32).T[HEAD_DIM:, :].astype(bf)
        kt_ref[:HEAD_DIM, b * step : (b + 1) * step] = kt
        kt_ref[HEAD_DIM : 2 * HEAD_DIM, b * step : (b + 1) * step] = kt
    b2 = bias_ref[...] * LOG2E
    b_high = b2.astype(bf).astype(jnp.float32)
    b_mid = (b2 - b_high).astype(bf).astype(jnp.float32)
    b_low = b2 - b_high - b_mid
    row = lax.broadcasted_iota(jnp.int32, (128, length), 0)
    tail = jnp.where(row == 0, b_high, jnp.where(row == 1, b_mid, jnp.where(row == 2, b_low, 0.0)))
    kt_ref[2 * HEAD_DIM :, :] = tail.astype(bf)

    below = lax.broadcasted_iota(jnp.int32, (bk, bk), 0) > lax.broadcasted_iota(jnp.int32, (bk, bk), 1)
    mask_ref[...] = jnp.where(below, 1.0, 0.0)
    tri_ref[...] = jnp.where(below, 1.0, 0.0).astype(bf)
    acc_ref[...] = jnp.zeros_like(acc_ref)
    car_ref[...] = jnp.zeros_like(car_ref)

    for c in reversed(range(length // bk)):
        at = c * bk
        x = jnp.dot(qa_ref[at:, :], kt_ref[:, at : at + bk], preferred_element_type=jnp.float32)
        soft = jnp.maximum(x, jnp.log2(1.0 + jnp.exp2(jnp.minimum(x, 126.0))))
        own = x - soft
        soft = masked(soft, mask_ref[...])
        after = jnp.dot(soft.astype(bf), tri_ref[...], preferred_element_type=jnp.float32)
        a = masked(jnp.exp2(own - after), mask_ref[...])
        carry = car_ref[at:, :]
        here = jnp.dot(a.astype(bf), v_ref[at : at + bk, :], preferred_element_type=jnp.float32)
        acc_ref[at:, :] += here * jnp.exp2(-carry)[:, :HEAD_DIM]
        total = after[:, :128] + soft[:, :128]
        car_ref[at:, :] = carry + jnp.broadcast_to(total[:, :1], carry.shape)

    for b in range(src):
        att = acc_ref[b * rows : (b + 1) * rows, :]
        scaled = att * lax.rsqrt(jnp.mean(att * att, axis=1, keepdims=True) + norm_eps) * gain_ref[...]
        head = scaled.astype(bf)
        out_ref[b] = jnp.concatenate([head[:half], head[half:]], axis=1)


def output_kernel(got_ref, own_ref, far_ref, out_ref, heads_ref):
    x, c, z, y = place_of()
    half = got_ref.shape[1]
    for h in range(SIDE * SIDE):
        block = got_ref[h]
        heads_ref[:half, h * HEAD_DIM : (h + 1) * HEAD_DIM] = block[:, :HEAD_DIM]
        heads_ref[half:, h * HEAD_DIM : (h + 1) * HEAD_DIM] = block[:, HEAD_DIM:]
    for i in range(SIDE):
        for cc, ref in ((0, own_ref), (1, far_ref)):
            parts = [
                ref[i, before(z, zs), jnp.bitwise_xor(y, ys)] for zs in range(SIDE) for ys in range(SIDE)
            ]
            mixed = jnp.dot(
                heads_ref[...], jnp.concatenate(parts, axis=0), preferred_element_type=jnp.float32
            )
            chunk = 2 * before(x, i) + jnp.bitwise_xor(c, cc)
            out_ref[:, pl.ds(pl.multiple_of(chunk * 256, 256), 256)] = mixed.astype(jnp.bfloat16)


def body(inputs, in_gain, w_query, w_key, w_value, key_bias, out_gain, w_out):
    bf = jnp.bfloat16
    rows, width = inputs.shape[1], inputs.shape[2]
    sp_size = lax.axis_size("sp")
    sp = lax.axis_index("sp")

    wide = inputs[0].astype(jnp.float32)
    normed = (
        wide * lax.rsqrt(jnp.mean(wide * wide, axis=-1, keepdims=True) + norm_eps) * in_gain
    ).astype(bf)

    def spread(perm_of, a, axis):
        return [a] + [lax.ppermute(a, axis, perm_of(k)) for k in range(1, SIDE)]

    piece = jnp.concatenate([w_query.T, w_key.T, w_value.T], axis=0)
    four = doubled(piece[None], "dp", (pairs(2, 8), pairs(4, 8)))
    together = jnp.concatenate([four[:2].reshape(192, 256), w_out], axis=0)[None]
    first_a = doubled(together, "sp", (pairs(1, 16), pairs(2, 16)))
    first_b = doubled(four[2:][None], "sp", (pairs(4, 16), pairs(8, 16)))
    rest_y = first_a[:, 192:]
    first_a = first_a[:, :192].reshape(SIDE, 2, 96, 256)
    first_a, first_b, normed = lax.optimization_barrier((first_a, first_b, normed))
    own_a = jnp.stack(spread(lambda k: along_zy(k, 0), first_a, "sp"))
    own_b = jnp.stack(spread(lambda k: along_zy(0, k), first_b, "sp"))
    own_a, rest_y = lax.optimization_barrier((own_a, rest_y))
    far_a = lax.ppermute(own_a, "dp", pairs(1, 8))
    far_b = lax.ppermute(own_b, "dp", pairs(1, 8))
    packed, done = pl.pallas_call(
        project_kernel,
        out_shape=(
            pltpu.VMEM((sp_size, rows + rows // 2, 128), bf),
            jax.ShapeDtypeStruct((8, 128), jnp.float32),
        ),
        in_specs=[VMEM] * 5,
        out_specs=(VMEM, VMEM),
        scratch_shapes=[pltpu.VMEM((rows, width), bf), pltpu.VMEM((sp_size, 96, rows), jnp.float32)],
        compiler_params=pltpu.CompilerParams(vmem_limit_bytes=30 * 2**20),
        name="project",
    )(*near(normed, own_a, own_b, far_a, far_b))
    rest_z = spread(lambda k: along_zy(k, 0), rest_y, "sp")
    _, rest_z = lax.optimization_barrier((done, rest_z))
    rest_x = spread(along_x, jnp.stack(rest_z), "dp")

    got = lax.all_to_all(packed, "sp", split_axis=0, concat_axis=0, tiled=True)
    gains = lax.dynamic_slice_in_dim(out_gain, sp * HEAD_DIM, HEAD_DIM, 0)[None]
    length = sp_size * rows
    bk = 256
    heads = pl.pallas_call(
        functools.partial(attend_kernel, src=sp_size, rows=rows, bk=bk),
        out_shape=pltpu.VMEM((sp_size, rows // 2, 128), bf),
        in_specs=[VMEM] * 3,
        out_specs=VMEM,
        scratch_shapes=[
            pltpu.VMEM((length, 256), bf),
            pltpu.VMEM((256, length), bf),
            pltpu.VMEM((length, HEAD_DIM), bf),
            pltpu.VMEM((length, HEAD_DIM), jnp.float32),
            pltpu.VMEM((length, 128), jnp.float32),
            pltpu.VMEM((bk, bk), jnp.float32),
            pltpu.VMEM((bk, bk), bf),
        ],
        compiler_params=pltpu.CompilerParams(vmem_limit_bytes=30 * 2**20),
        name="attend",
    )(*near(got, key_bias.reshape(1, length), gains))
    heads, rest_x = lax.optimization_barrier((heads, rest_x))
    own_out = jnp.stack(rest_x)
    far_out = lax.ppermute(own_out, "dp", pairs(1, 8))
    returned = lax.all_to_all(heads, "sp", split_axis=0, concat_axis=0, tiled=True)
    mixed = pl.pallas_call(
        output_kernel,
        out_shape=jax.ShapeDtypeStruct((rows, width), bf),
        in_specs=[VMEM] * 3,
        out_specs=VMEM,
        scratch_shapes=[pltpu.VMEM((rows, sp_size * HEAD_DIM), bf)],
        compiler_params=pltpu.CompilerParams(vmem_limit_bytes=30 * 2**20),
        name="output",
    )(*near(returned, own_out, far_out))
    return mixed[None]


def solution(mesh):
    placed = (
        P("dp", "sp", None),
        P(),
        P("dp", "sp"),
        P("dp", "sp"),
        P("dp", "sp"),
        P("dp", None, "sp"),
        P(),
        P("sp", "dp"),
    )

    return jax.shard_map(body, mesh=mesh, in_specs=placed, out_specs=P("dp", "sp", None), check_vma=False)
```

```python
import functools
import math

import jax
import jax.numpy as jnp
from jax import lax
from jax.experimental import pallas as pl
from jax.experimental.pallas import tpu as pltpu
from jax.sharding import PartitionSpec as P

HEAD_DIM = 64
LOG2E = math.log2(math.e)
norm_eps = 1e-06
SIDE = 4


VMEM = pl.BlockSpec(memory_space=pltpu.VMEM)


def pairs(step, size):
    return [(i, i ^ step) for i in range(size)]


def along_x(k):
    return [(i, (i + 2 * k) % (2 * SIDE)) for i in range(2 * SIDE)]


def along_zy(dz, dy):
    return [
        (s, ((s // SIDE + dz) % SIDE) * SIDE + (s % SIDE + dy) % SIDE) for s in range(SIDE * SIDE)
    ]


def near(*arrays):
    return [pltpu.with_memory_space_constraint(a, pltpu.VMEM) for a in arrays]


def place_of():
    dp, sp = lax.axis_index("dp"), lax.axis_index("sp")
    return lax.div(dp, 2), lax.rem(dp, 2), lax.div(sp, SIDE), lax.rem(sp, SIDE)


def before(here, there):
    return lax.rem(here + SIDE - there, SIDE)


def project_kernel(normed_ref, own_a, own_b, far_a, far_b, out_ref, done_ref, order_ref, sums_ref):
    bf = jnp.bfloat16
    x, c, z, y = place_of()
    rows = normed_ref.shape[0]
    for i in range(SIDE):
        for cc in range(2):
            chunk = 2 * jnp.bitwise_xor(x, i) + jnp.bitwise_xor(c, cc)
            order_ref[:, (2 * i + cc) * 256 : (2 * i + cc + 1) * 256] = normed_ref[
                :, pl.ds(pl.multiple_of(chunk * 256, 256), 256)
            ]
    for zs in range(SIDE):
        parts = []
        for i in range(SIDE):
            for ref_a, ref_b in ((own_a, own_b), (far_a, far_b)):
                if i < 2:
                    several = [ref_a[before(z, zs), before(y, ys), i] for ys in range(SIDE)]
                else:
                    several = [ref_b[before(y, ys), before(z, zs), i - 2] for ys in range(SIDE)]
                parts.append(jnp.concatenate(several, axis=0))
        weights = jnp.concatenate(parts, axis=1)
        total = lax.dot_general(
            weights, order_ref[...], (((1,), (1,)), ((), ())), preferred_element_type=jnp.float32
        )
        for ys in range(SIDE):
            sums_ref[SIDE * zs + ys] = total[96 * ys : 96 * (ys + 1), :]
    half = rows // 2
    for g in range(SIDE):
        key = jnp.concatenate([sums_ref[SIDE * g + j, 64:80, :] for j in range(SIDE)], axis=0)
        value = jnp.concatenate([sums_ref[SIDE * g + j, 80:96, :] for j in range(SIDE)], axis=0)
        turned = value.T.astype(bf)
        for j in range(SIDE):
            h = SIDE * g + j
            both = jnp.concatenate([sums_ref[h, :64, :], key], axis=0)
            out_ref[h, :rows, :] = both.T.astype(bf)
            out_ref[h, rows:, :] = jnp.concatenate([turned[:half], turned[half:]], axis=1)
    done_ref[...] = jnp.zeros_like(done_ref)


def masked(block, mask):
    rows = mask.shape[0]
    first = block[:rows] * mask
    return first if block.shape[0] == rows else jnp.concatenate([first, block[rows:]], axis=0)


def attend_kernel(
    got_ref, bias_ref, gain_ref, out_ref, qa_ref, kt_ref, v_ref, acc_ref, car_ref, mask_ref, tri_ref, *, src, rows, bk
):
    bf = jnp.bfloat16
    half = rows // 2
    length = src * rows
    lane = lax.broadcasted_iota(jnp.int32, (rows, 128), 1)
    ones = jnp.where(lane < 3, 1.0, 0.0).astype(bf)
    for b in range(src):
        both = got_ref[b, :rows, :]
        wide = both[:, :HEAD_DIM].astype(jnp.float32) * (LOG2E * HEAD_DIM ** -0.5)
        high = wide.astype(bf)
        low = (wide - high.astype(jnp.float32)).astype(bf)
        qa_ref[b * rows : (b + 1) * rows, :128] = jnp.concatenate([high, low], axis=1)
        qa_ref[b * rows : (b + 1) * rows, 128:] = ones
        vv = got_ref[b, rows:, :]
        v_ref[b * rows : b * rows + half, :] = vv[:, :HEAD_DIM]
        v_ref[b * rows + half : (b + 1) * rows, :] = vv[:, HEAD_DIM:]
    step = 2 * rows
    for b in range(src // 2):
        pair = jnp.concatenate([got_ref[2 * b, :rows, :], got_ref[2 * b + 1, :rows, :]], axis=0)
        kt = pair.astype(jnp.float32).T[HEAD_DIM:, :].astype(bf)
        kt_ref[:HEAD_DIM, b * step : (b + 1) * step] = kt
        kt_ref[HEAD_DIM : 2 * HEAD_DIM, b * step : (b + 1) * step] = kt
    b2 = bias_ref[...] * LOG2E
    b_high = b2.astype(bf).astype(jnp.float32)
    b_mid = (b2 - b_high).astype(bf).astype(jnp.float32)
    b_low = b2 - b_high - b_mid
    row = lax.broadcasted_iota(jnp.int32, (128, length), 0)
    tail = jnp.where(row == 0, b_high, jnp.where(row == 1, b_mid, jnp.where(row == 2, b_low, 0.0)))
    kt_ref[2 * HEAD_DIM :, :] = tail.astype(bf)

    below = lax.broadcasted_iota(jnp.int32, (bk, bk), 0) > lax.broadcasted_iota(jnp.int32, (bk, bk), 1)
    mask_ref[...] = jnp.where(below, 1.0, 0.0)
    tri_ref[...] = jnp.where(below, 1.0, 0.0).astype(bf)
    acc_ref[...] = jnp.zeros_like(acc_ref)
    car_ref[...] = jnp.zeros_like(car_ref)

    for c in reversed(range(length // bk)):
        at = c * bk
        x = jnp.dot(qa_ref[at:, :], kt_ref[:, at : at + bk], preferred_element_type=jnp.float32)
        soft = jnp.maximum(x, jnp.log2(1.0 + jnp.exp2(jnp.minimum(x, 126.0))))
        own = x - soft
        soft = masked(soft, mask_ref[...])
        after = jnp.dot(soft.astype(bf), tri_ref[...], preferred_element_type=jnp.float32)
        a = masked(jnp.exp2(own - after), mask_ref[...])
        carry = car_ref[at:, :]
        here = jnp.dot(a.astype(bf), v_ref[at : at + bk, :], preferred_element_type=jnp.float32)
        acc_ref[at:, :] += here * jnp.exp2(-carry)[:, :HEAD_DIM]
        total = after[:, :128] + soft[:, :128]
        car_ref[at:, :] = carry + jnp.broadcast_to(total[:, :1], carry.shape)

    for b in range(src):
        att = acc_ref[b * rows : (b + 1) * rows, :]
        scaled = att * lax.rsqrt(jnp.mean(att * att, axis=1, keepdims=True) + norm_eps) * gain_ref[...]
        head = scaled.astype(bf)
        out_ref[b] = jnp.concatenate([head[:half], head[half:]], axis=1)


def output_kernel(got_ref, own_ref, far_ref, out_ref, heads_ref):
    x, c, z, y = place_of()
    half = got_ref.shape[1]
    for h in range(SIDE * SIDE):
        block = got_ref[h]
        heads_ref[:half, h * HEAD_DIM : (h + 1) * HEAD_DIM] = block[:, :HEAD_DIM]
        heads_ref[half:, h * HEAD_DIM : (h + 1) * HEAD_DIM] = block[:, HEAD_DIM:]
    for i in range(SIDE):
        for cc, ref in ((0, own_ref), (1, far_ref)):
            parts = [
                ref[i, before(z, zs), before(y, ys)] for zs in range(SIDE) for ys in range(SIDE)
            ]
            mixed = jnp.dot(
                heads_ref[...], jnp.concatenate(parts, axis=0), preferred_element_type=jnp.float32
            )
            chunk = 2 * before(x, i) + jnp.bitwise_xor(c, cc)
            out_ref[:, pl.ds(pl.multiple_of(chunk * 256, 256), 256)] = mixed.astype(jnp.bfloat16)


def body(inputs, in_gain, w_query, w_key, w_value, key_bias, out_gain, w_out):
    bf = jnp.bfloat16
    rows, width = inputs.shape[1], inputs.shape[2]
    sp_size = lax.axis_size("sp")
    sp = lax.axis_index("sp")

    wide = inputs[0].astype(jnp.float32)
    normed = (
        wide * lax.rsqrt(jnp.mean(wide * wide, axis=-1, keepdims=True) + norm_eps) * in_gain
    ).astype(bf)

    def spread(perm_of, a, axis):
        return [a] + [lax.ppermute(a, axis, perm_of(k)) for k in range(1, SIDE)]

    piece = jnp.concatenate([w_query.T, w_key.T, w_value.T], axis=0)
    two = jnp.stack([piece, lax.ppermute(piece, "dp", pairs(2, 8))])
    four = lax.ppermute(two, "dp", pairs(4, 8))
    together = jnp.concatenate([two.reshape(192, 256), w_out], axis=0)
    first_a = spread(lambda k: along_zy(0, k), together, "sp")
    first_a = jnp.stack(first_a)
    first_b = jnp.stack(spread(lambda k: along_zy(k, 0), four, "sp"))
    rest_y = first_a[:, 192:]
    first_a = first_a[:, :192].reshape(SIDE, 2, 96, 256)
    first_a, first_b, rest_y = lax.optimization_barrier((first_a, first_b, rest_y))
    own_b = spread(lambda k: along_zy(0, k), first_b, "sp")
    own_a = spread(lambda k: along_zy(k, 0), first_a, "sp")
    rest_z = spread(lambda k: along_zy(k, 0), rest_y, "sp")
    own_b = jnp.stack(own_b)
    own_a = jnp.stack(own_a)
    far_a = lax.ppermute(own_a, "dp", pairs(1, 8))
    far_b = lax.ppermute(own_b, "dp", pairs(1, 8))
    packed, done = pl.pallas_call(
        project_kernel,
        out_shape=(
            pltpu.VMEM((sp_size, rows + rows // 2, 128), bf),
            jax.ShapeDtypeStruct((8, 128), jnp.float32),
        ),
        in_specs=[VMEM] * 5,
        out_specs=(VMEM, VMEM),
        scratch_shapes=[pltpu.VMEM((rows, width), bf), pltpu.VMEM((sp_size, 96, rows), jnp.float32)],
        compiler_params=pltpu.CompilerParams(vmem_limit_bytes=30 * 2**20),
        name="project",
    )(*near(normed, own_a, own_b, far_a, far_b))
    _, rest_z = lax.optimization_barrier((done, rest_z))
    rest_x = spread(along_x, jnp.stack(rest_z), "dp")

    got = lax.all_to_all(packed, "sp", split_axis=0, concat_axis=0, tiled=True)
    gains = lax.dynamic_slice_in_dim(out_gain, sp * HEAD_DIM, HEAD_DIM, 0)[None]
    length = sp_size * rows
    bk = 256
    heads = pl.pallas_call(
        functools.partial(attend_kernel, src=sp_size, rows=rows, bk=bk),
        out_shape=pltpu.VMEM((sp_size, rows // 2, 128), bf),
        in_specs=[VMEM] * 3,
        out_specs=VMEM,
        scratch_shapes=[
            pltpu.VMEM((length, 256), bf),
            pltpu.VMEM((256, length), bf),
            pltpu.VMEM((length, HEAD_DIM), bf),
            pltpu.VMEM((length, HEAD_DIM), jnp.float32),
            pltpu.VMEM((length, 128), jnp.float32),
            pltpu.VMEM((bk, bk), jnp.float32),
            pltpu.VMEM((bk, bk), bf),
        ],
        compiler_params=pltpu.CompilerParams(vmem_limit_bytes=30 * 2**20),
        name="attend",
    )(*near(got, key_bias.reshape(1, length), gains))
    heads, rest_x = lax.optimization_barrier((heads, rest_x))
    own_out = jnp.stack(rest_x)
    far_out = lax.ppermute(own_out, "dp", pairs(1, 8))
    returned = lax.all_to_all(heads, "sp", split_axis=0, concat_axis=0, tiled=True)
    mixed = pl.pallas_call(
        output_kernel,
        out_shape=jax.ShapeDtypeStruct((rows, width), bf),
        in_specs=[VMEM] * 3,
        out_specs=VMEM,
        scratch_shapes=[pltpu.VMEM((rows, sp_size * HEAD_DIM), bf)],
        compiler_params=pltpu.CompilerParams(vmem_limit_bytes=30 * 2**20),
        name="output",
    )(*near(returned, own_out, far_out))
    return mixed[None]


def solution(mesh):
    placed = (
        P("dp", "sp", None),
        P(),
        P("dp", "sp"),
        P("dp", "sp"),
        P("dp", "sp"),
        P("dp", None, "sp"),
        P(),
        P("sp", "dp"),
    )

    return jax.shard_map(
        body, mesh=mesh, in_specs=placed, out_specs=P("dp", "sp", None), check_vma=False
    )
```

```python
import functools
import math

import jax
import jax.numpy as jnp
from jax import lax
from jax.experimental import pallas as pl
from jax.experimental.pallas import tpu as pltpu
from jax.sharding import PartitionSpec as P

HEAD_DIM = 64
LOG2E = math.log2(math.e)
norm_eps = 1e-06
SIDE = 4
ARRIVAL = (0, 1, 3, 2)


VMEM = pl.BlockSpec(memory_space=pltpu.VMEM)


def pairs(step, size):
    return [(i, i ^ step) for i in range(size)]


def along_x(k):
    return [(i, (i + 2 * k) % (2 * SIDE)) for i in range(2 * SIDE)]


def along_zy(dz, dy):
    return [
        (s, ((s // SIDE + dz) % SIDE) * SIDE + (s % SIDE + dy) % SIDE) for s in range(SIDE * SIDE)
    ]


def near(*arrays):
    return [pltpu.with_memory_space_constraint(a, pltpu.VMEM) for a in arrays]


def place_of():
    dp, sp = lax.axis_index("dp"), lax.axis_index("sp")
    return lax.div(dp, 2), lax.rem(dp, 2), lax.div(sp, SIDE), lax.rem(sp, SIDE)


def before(here, there):
    return lax.rem(here + SIDE - there, SIDE)


def project_kernel(normed_ref, *refs):
    own_a, own_b, far_a, far_b = (
        {k: refs[at + 2 * i] for i, k in enumerate(ARRIVAL)} for at in (0, 1, 2 * SIDE, 2 * SIDE + 1)
    )
    out_ref, done_ref, order_ref, sums_ref = refs[4 * SIDE :]
    bf = jnp.bfloat16
    x, c, z, y = place_of()
    rows = normed_ref.shape[0]
    for i in range(SIDE):
        for cc in range(2):
            chunk = 2 * jnp.bitwise_xor(x, i) + jnp.bitwise_xor(c, cc)
            order_ref[:, (2 * i + cc) * 256 : (2 * i + cc + 1) * 256] = normed_ref[
                :, pl.ds(pl.multiple_of(chunk * 256, 256), 256)
            ]
    for kz in range(SIDE):
        parts = []
        for i in range(SIDE):
            for refs_a, refs_b in ((own_a, own_b), (far_a, far_b)):
                if i < 2:
                    several = [refs_a[kz][ky, i] for ky in range(SIDE)]
                else:
                    several = [refs_b[ky][kz, i - 2] for ky in range(SIDE)]
                parts.append(jnp.concatenate(several, axis=0))
        weights = jnp.concatenate(parts, axis=1)
        total = lax.dot_general(
            weights, order_ref[...], (((1,), (1,)), ((), ())), preferred_element_type=jnp.float32
        )
        for ky in range(SIDE):
            sums_ref[SIDE * before(z, kz) + before(y, ky)] = total[96 * ky : 96 * (ky + 1), :]
    half = rows // 2
    for g in range(SIDE):
        key = jnp.concatenate([sums_ref[SIDE * g + j, 64:80, :] for j in range(SIDE)], axis=0)
        value = jnp.concatenate([sums_ref[SIDE * g + j, 80:96, :] for j in range(SIDE)], axis=0)
        turned = value.T.astype(bf)
        for j in range(SIDE):
            h = SIDE * g + j
            both = jnp.concatenate([sums_ref[h, :64, :], key], axis=0)
            out_ref[h, :rows, :] = both.T.astype(bf)
            out_ref[h, rows:, :] = jnp.concatenate([turned[:half], turned[half:]], axis=1)
    done_ref[...] = jnp.zeros_like(done_ref)


def masked(block, mask):
    rows = mask.shape[0]
    first = block[:rows] * mask
    return first if block.shape[0] == rows else jnp.concatenate([first, block[rows:]], axis=0)


def attend_kernel(
    got_ref, bias_ref, gain_ref, out_ref, qa_ref, kt_ref, v_ref, acc_ref, car_ref, mask_ref, tri_ref, *, src, rows, bk
):
    bf = jnp.bfloat16
    half = rows // 2
    length = src * rows
    lane = lax.broadcasted_iota(jnp.int32, (rows, 128), 1)
    ones = jnp.where(lane < 3, 1.0, 0.0).astype(bf)
    for b in range(src):
        both = got_ref[b, :rows, :]
        wide = both[:, :HEAD_DIM].astype(jnp.float32) * (LOG2E * HEAD_DIM ** -0.5)
        high = wide.astype(bf)
        low = (wide - high.astype(jnp.float32)).astype(bf)
        qa_ref[b * rows : (b + 1) * rows, :128] = jnp.concatenate([high, low], axis=1)
        qa_ref[b * rows : (b + 1) * rows, 128:] = ones
        vv = got_ref[b, rows:, :]
        v_ref[b * rows : b * rows + half, :] = vv[:, :HEAD_DIM]
        v_ref[b * rows + half : (b + 1) * rows, :] = vv[:, HEAD_DIM:]
    step = 2 * rows
    for b in range(src // 2):
        pair = jnp.concatenate([got_ref[2 * b, :rows, :], got_ref[2 * b + 1, :rows, :]], axis=0)
        kt = pair.astype(jnp.float32).T[HEAD_DIM:, :].astype(bf)
        kt_ref[:HEAD_DIM, b * step : (b + 1) * step] = kt
        kt_ref[HEAD_DIM : 2 * HEAD_DIM, b * step : (b + 1) * step] = kt
    b2 = bias_ref[...] * LOG2E
    b_high = b2.astype(bf).astype(jnp.float32)
    b_mid = (b2 - b_high).astype(bf).astype(jnp.float32)
    b_low = b2 - b_high - b_mid
    row = lax.broadcasted_iota(jnp.int32, (128, length), 0)
    tail = jnp.where(row == 0, b_high, jnp.where(row == 1, b_mid, jnp.where(row == 2, b_low, 0.0)))
    kt_ref[2 * HEAD_DIM :, :] = tail.astype(bf)

    below = lax.broadcasted_iota(jnp.int32, (bk, bk), 0) > lax.broadcasted_iota(jnp.int32, (bk, bk), 1)
    mask_ref[...] = jnp.where(below, 1.0, 0.0)
    tri_ref[...] = jnp.where(below, 1.0, 0.0).astype(bf)
    acc_ref[...] = jnp.zeros_like(acc_ref)
    car_ref[...] = jnp.zeros_like(car_ref)

    for c in reversed(range(length // bk)):
        at = c * bk
        x = jnp.dot(qa_ref[at:, :], kt_ref[:, at : at + bk], preferred_element_type=jnp.float32)
        soft = jnp.maximum(x, jnp.log2(1.0 + jnp.exp2(jnp.minimum(x, 126.0))))
        own = x - soft
        soft = masked(soft, mask_ref[...])
        after = jnp.dot(soft.astype(bf), tri_ref[...], preferred_element_type=jnp.float32)
        a = masked(jnp.exp2(own - after), mask_ref[...])
        carry = car_ref[at:, :]
        here = jnp.dot(a.astype(bf), v_ref[at : at + bk, :], preferred_element_type=jnp.float32)
        acc_ref[at:, :] += here * jnp.exp2(-carry)[:, :HEAD_DIM]
        total = after[:, :128] + soft[:, :128]
        car_ref[at:, :] = carry + jnp.broadcast_to(total[:, :1], carry.shape)

    for b in range(src):
        att = acc_ref[b * rows : (b + 1) * rows, :]
        scaled = att * lax.rsqrt(jnp.mean(att * att, axis=1, keepdims=True) + norm_eps) * gain_ref[...]
        head = scaled.astype(bf)
        out_ref[b] = jnp.concatenate([head[:half], head[half:]], axis=1)


def output_kernel(got_ref, own_ref, far_ref, out_ref, heads_ref):
    x, c, z, y = place_of()
    half = got_ref.shape[1]
    for h in range(SIDE * SIDE):
        block = got_ref[h]
        heads_ref[:half, h * HEAD_DIM : (h + 1) * HEAD_DIM] = block[:, :HEAD_DIM]
        heads_ref[half:, h * HEAD_DIM : (h + 1) * HEAD_DIM] = block[:, HEAD_DIM:]
    for i in range(SIDE):
        for cc, ref in ((0, own_ref), (1, far_ref)):
            parts = [
                ref[i, before(z, zs), before(y, ys)] for zs in range(SIDE) for ys in range(SIDE)
            ]
            mixed = jnp.dot(
                heads_ref[...], jnp.concatenate(parts, axis=0), preferred_element_type=jnp.float32
            )
            chunk = 2 * before(x, i) + jnp.bitwise_xor(c, cc)
            out_ref[:, pl.ds(pl.multiple_of(chunk * 256, 256), 256)] = mixed.astype(jnp.bfloat16)


def body(inputs, in_gain, w_query, w_key, w_value, key_bias, out_gain, w_out):
    bf = jnp.bfloat16
    rows, width = inputs.shape[1], inputs.shape[2]
    sp_size = lax.axis_size("sp")
    sp = lax.axis_index("sp")

    wide = inputs[0].astype(jnp.float32)
    normed = (
        wide * lax.rsqrt(jnp.mean(wide * wide, axis=-1, keepdims=True) + norm_eps) * in_gain
    ).astype(bf)

    def spread(perm_of, a, axis):
        return [a] + [lax.ppermute(a, axis, perm_of(k)) for k in range(1, SIDE)]

    piece = jnp.concatenate([w_query.T, w_key.T, w_value.T], axis=0)
    two = jnp.stack([piece, lax.ppermute(piece, "dp", pairs(2, 8))])
    four = lax.ppermute(two, "dp", pairs(4, 8))
    together = jnp.concatenate([two.reshape(192, 256), w_out], axis=0)
    first_a = spread(lambda k: along_zy(0, k), together, "sp")
    first_a = jnp.stack(first_a)
    first_b = jnp.stack(spread(lambda k: along_zy(k, 0), four, "sp"))
    rest_y = first_a[:, 192:]
    first_a = first_a[:, :192].reshape(SIDE, 2, 96, 256)
    first_a, first_b, rest_y = lax.optimization_barrier((first_a, first_b, rest_y))
    own_a, own_b = {0: first_a}, {0: first_b}
    for k in ARRIVAL[1:]:
        own_a[k] = lax.ppermute(first_a, "sp", along_zy(k, 0))
        own_b[k] = lax.ppermute(first_b, "sp", along_zy(0, k))
    rest_z = spread(lambda k: along_zy(k, 0), rest_y, "sp")
    own = [group[k] for k in ARRIVAL for group in (own_a, own_b)]
    far = [lax.ppermute(block, "dp", pairs(1, 8)) for block in own]
    packed, done = pl.pallas_call(
        project_kernel,
        out_shape=(
            pltpu.VMEM((sp_size, rows + rows // 2, 128), bf),
            jax.ShapeDtypeStruct((8, 128), jnp.float32),
        ),
        in_specs=[VMEM] * (1 + 4 * SIDE),
        out_specs=(VMEM, VMEM),
        scratch_shapes=[pltpu.VMEM((rows, width), bf), pltpu.VMEM((sp_size, 96, rows), jnp.float32)],
        compiler_params=pltpu.CompilerParams(vmem_limit_bytes=30 * 2**20),
        name="project",
    )(*near(normed, *own, *far))
    _, rest_z = lax.optimization_barrier((done, rest_z))
    rest_x = spread(along_x, jnp.stack(rest_z), "dp")

    got = lax.all_to_all(packed, "sp", split_axis=0, concat_axis=0, tiled=True)
    gains = lax.dynamic_slice_in_dim(out_gain, sp * HEAD_DIM, HEAD_DIM, 0)[None]
    length = sp_size * rows
    bk = 256
    heads = pl.pallas_call(
        functools.partial(attend_kernel, src=sp_size, rows=rows, bk=bk),
        out_shape=pltpu.VMEM((sp_size, rows // 2, 128), bf),
        in_specs=[VMEM] * 3,
        out_specs=VMEM,
        scratch_shapes=[
            pltpu.VMEM((length, 256), bf),
            pltpu.VMEM((256, length), bf),
            pltpu.VMEM((length, HEAD_DIM), bf),
            pltpu.VMEM((length, HEAD_DIM), jnp.float32),
            pltpu.VMEM((length, 128), jnp.float32),
            pltpu.VMEM((bk, bk), jnp.float32),
            pltpu.VMEM((bk, bk), bf),
        ],
        compiler_params=pltpu.CompilerParams(vmem_limit_bytes=30 * 2**20),
        name="attend",
    )(*near(got, key_bias.reshape(1, length), gains))
    heads, rest_x = lax.optimization_barrier((heads, rest_x))
    own_out = jnp.stack(rest_x)
    far_out = lax.ppermute(own_out, "dp", pairs(1, 8))
    returned = lax.all_to_all(heads, "sp", split_axis=0, concat_axis=0, tiled=True)
    mixed = pl.pallas_call(
        output_kernel,
        out_shape=jax.ShapeDtypeStruct((rows, width), bf),
        in_specs=[VMEM] * 3,
        out_specs=VMEM,
        scratch_shapes=[pltpu.VMEM((rows, sp_size * HEAD_DIM), bf)],
        compiler_params=pltpu.CompilerParams(vmem_limit_bytes=30 * 2**20),
        name="output",
    )(*near(returned, own_out, far_out))
    return mixed[None]


def solution(mesh):
    placed = (
        P("dp", "sp", None),
        P(),
        P("dp", "sp"),
        P("dp", "sp"),
        P("dp", "sp"),
        P("dp", None, "sp"),
        P(),
        P("sp", "dp"),
    )

    return jax.shard_map(
        body, mesh=mesh, in_specs=placed, out_specs=P("dp", "sp", None), check_vma=False
    )
```

```python
import functools
import math

import jax
import jax.numpy as jnp
from jax import lax
from jax.experimental import pallas as pl
from jax.experimental.pallas import tpu as pltpu
from jax.sharding import PartitionSpec as P

HEAD_DIM = 64
LOG2E = math.log2(math.e)
norm_eps = 1e-06
SIDE = 4


VMEM = pl.BlockSpec(memory_space=pltpu.VMEM)


def pairs(step, size):
    return [(i, i ^ step) for i in range(size)]


def along_x(k):
    return [(i, (i + 2 * k) % (2 * SIDE)) for i in range(2 * SIDE)]


def along_zy(dz, dy):
    return [
        (s, ((s // SIDE + dz) % SIDE) * SIDE + (s % SIDE + dy) % SIDE) for s in range(SIDE * SIDE)
    ]


def near(*arrays):
    return [pltpu.with_memory_space_constraint(a, pltpu.VMEM) for a in arrays]


def place_of():
    dp, sp = lax.axis_index("dp"), lax.axis_index("sp")
    return lax.div(dp, 2), lax.rem(dp, 2), lax.div(sp, SIDE), lax.rem(sp, SIDE)


def before(here, there):
    return lax.rem(here + SIDE - there, SIDE)


def project_kernel(normed_ref, *refs):
    own_a, own_b, far_a, far_b = (refs[SIDE * i : SIDE * (i + 1)] for i in range(4))
    out_ref, done_ref, order_ref, sums_ref = refs[4 * SIDE :]
    bf = jnp.bfloat16
    x, c, z, y = place_of()
    rows = normed_ref.shape[0]
    for i in range(SIDE):
        for cc in range(2):
            chunk = 2 * jnp.bitwise_xor(x, i) + jnp.bitwise_xor(c, cc)
            order_ref[:, (2 * i + cc) * 256 : (2 * i + cc + 1) * 256] = normed_ref[
                :, pl.ds(pl.multiple_of(chunk * 256, 256), 256)
            ]
    for kz in range(SIDE):
        parts = []
        for i in range(SIDE):
            for refs_a, refs_b in ((own_a, own_b), (far_a, far_b)):
                several = []
                for ky in range(SIDE):
                    if i == 0:
                        several.append(refs_a[kz][ky, :96])
                    elif i == 1:
                        several += [refs_a[kz][ky, 96:], refs_b[ky][kz, :32]]
                    else:
                        several.append(refs_b[ky][kz, 96 * i - 160 : 96 * i - 64])
                parts.append(jnp.concatenate(several, axis=0))
        weights = jnp.concatenate(parts, axis=1)
        total = lax.dot_general(
            weights, order_ref[...], (((1,), (1,)), ((), ())), preferred_element_type=jnp.float32
        )
        for ky in range(SIDE):
            sums_ref[SIDE * before(z, kz) + before(y, ky)] = total[96 * ky : 96 * (ky + 1), :]
    half = rows // 2
    for g in range(SIDE):
        key = jnp.concatenate([sums_ref[SIDE * g + j, 64:80, :] for j in range(SIDE)], axis=0)
        value = jnp.concatenate([sums_ref[SIDE * g + j, 80:96, :] for j in range(SIDE)], axis=0)
        turned = value.T.astype(bf)
        for j in range(SIDE):
            h = SIDE * g + j
            both = jnp.concatenate([sums_ref[h, :64, :], key], axis=0)
            out_ref[h, :rows, :] = both.T.astype(bf)
            out_ref[h, rows:, :] = jnp.concatenate([turned[:half], turned[half:]], axis=1)
    done_ref[...] = jnp.zeros_like(done_ref)


def masked(block, mask):
    rows = mask.shape[0]
    first = block[:rows] * mask
    return first if block.shape[0] == rows else jnp.concatenate([first, block[rows:]], axis=0)


def attend_kernel(
    got_ref, bias_ref, gain_ref, out_ref, qa_ref, kt_ref, v_ref, acc_ref, car_ref, mask_ref, tri_ref, *, src, rows, bk
):
    bf = jnp.bfloat16
    half = rows // 2
    length = src * rows
    lane = lax.broadcasted_iota(jnp.int32, (rows, 128), 1)
    ones = jnp.where(lane < 3, 1.0, 0.0).astype(bf)
    for b in range(src):
        both = got_ref[b, :rows, :]
        wide = both[:, :HEAD_DIM].astype(jnp.float32) * (LOG2E * HEAD_DIM ** -0.5)
        high = wide.astype(bf)
        low = (wide - high.astype(jnp.float32)).astype(bf)
        qa_ref[b * rows : (b + 1) * rows, :128] = jnp.concatenate([high, low], axis=1)
        qa_ref[b * rows : (b + 1) * rows, 128:] = ones
        vv = got_ref[b, rows:, :]
        v_ref[b * rows : b * rows + half, :] = vv[:, :HEAD_DIM]
        v_ref[b * rows + half : (b + 1) * rows, :] = vv[:, HEAD_DIM:]
    step = 2 * rows
    for b in range(src // 2):
        pair = jnp.concatenate([got_ref[2 * b, :rows, :], got_ref[2 * b + 1, :rows, :]], axis=0)
        kt = pair.astype(jnp.float32).T[HEAD_DIM:, :].astype(bf)
        kt_ref[:HEAD_DIM, b * step : (b + 1) * step] = kt
        kt_ref[HEAD_DIM : 2 * HEAD_DIM, b * step : (b + 1) * step] = kt
    b2 = bias_ref[...] * LOG2E
    b_high = b2.astype(bf).astype(jnp.float32)
    b_mid = (b2 - b_high).astype(bf).astype(jnp.float32)
    b_low = b2 - b_high - b_mid
    row = lax.broadcasted_iota(jnp.int32, (128, length), 0)
    tail = jnp.where(row == 0, b_high, jnp.where(row == 1, b_mid, jnp.where(row == 2, b_low, 0.0)))
    kt_ref[2 * HEAD_DIM :, :] = tail.astype(bf)

    below = lax.broadcasted_iota(jnp.int32, (bk, bk), 0) > lax.broadcasted_iota(jnp.int32, (bk, bk), 1)
    mask_ref[...] = jnp.where(below, 1.0, 0.0)
    tri_ref[...] = jnp.where(below, 1.0, 0.0).astype(bf)
    acc_ref[...] = jnp.zeros_like(acc_ref)
    car_ref[...] = jnp.zeros_like(car_ref)

    for c in reversed(range(length // bk)):
        at = c * bk
        x = jnp.dot(qa_ref[at:, :], kt_ref[:, at : at + bk], preferred_element_type=jnp.float32)
        soft = jnp.maximum(x, jnp.log2(1.0 + jnp.exp2(jnp.minimum(x, 126.0))))
        own = x - soft
        soft = masked(soft, mask_ref[...])
        after = jnp.dot(soft.astype(bf), tri_ref[...], preferred_element_type=jnp.float32)
        a = masked(jnp.exp2(own - after), mask_ref[...])
        carry = car_ref[at:, :]
        here = jnp.dot(a.astype(bf), v_ref[at : at + bk, :], preferred_element_type=jnp.float32)
        acc_ref[at:, :] += here * jnp.exp2(-carry)[:, :HEAD_DIM]
        total = after[:, :128] + soft[:, :128]
        car_ref[at:, :] = carry + jnp.broadcast_to(total[:, :1], carry.shape)

    for b in range(src):
        att = acc_ref[b * rows : (b + 1) * rows, :]
        scaled = att * lax.rsqrt(jnp.mean(att * att, axis=1, keepdims=True) + norm_eps) * gain_ref[...]
        head = scaled.astype(bf)
        out_ref[b] = jnp.concatenate([head[:half], head[half:]], axis=1)


def output_kernel(got_ref, own_ref, far_ref, out_ref, heads_ref):
    x, c, z, y = place_of()
    half = got_ref.shape[1]
    for h in range(SIDE * SIDE):
        block = got_ref[h]
        heads_ref[:half, h * HEAD_DIM : (h + 1) * HEAD_DIM] = block[:, :HEAD_DIM]
        heads_ref[half:, h * HEAD_DIM : (h + 1) * HEAD_DIM] = block[:, HEAD_DIM:]
    for i in range(SIDE):
        for cc, ref in ((0, own_ref), (1, far_ref)):
            parts = [
                ref[i, before(z, zs), before(y, ys)] for zs in range(SIDE) for ys in range(SIDE)
            ]
            mixed = jnp.dot(
                heads_ref[...], jnp.concatenate(parts, axis=0), preferred_element_type=jnp.float32
            )
            chunk = 2 * before(x, i) + jnp.bitwise_xor(c, cc)
            out_ref[:, pl.ds(pl.multiple_of(chunk * 256, 256), 256)] = mixed.astype(jnp.bfloat16)


def body(inputs, in_gain, w_query, w_key, w_value, key_bias, out_gain, w_out):
    bf = jnp.bfloat16
    rows, width = inputs.shape[1], inputs.shape[2]
    sp_size = lax.axis_size("sp")
    sp = lax.axis_index("sp")

    wide = inputs[0].astype(jnp.float32)
    normed = (
        wide * lax.rsqrt(jnp.mean(wide * wide, axis=-1, keepdims=True) + norm_eps) * in_gain
    ).astype(bf)

    def spread(perm_of, a, axis):
        return [a] + [lax.ppermute(a, axis, perm_of(k)) for k in range(1, SIDE)]

    piece = jnp.concatenate([w_query.T, w_key.T, w_value.T], axis=0)
    two = jnp.stack([piece, lax.ppermute(piece, "dp", pairs(2, 8))])
    four = lax.ppermute(two, "dp", pairs(4, 8))
    together = jnp.concatenate([two[0], two[1, :64], w_out], axis=0)
    together_b = jnp.concatenate([two[1, 64:], four.reshape(192, 256)], axis=0)
    first_a = spread(lambda k: along_zy(0, k), together, "sp")
    first_a = jnp.stack(first_a)
    first_b = jnp.stack(spread(lambda k: along_zy(k, 0), together_b, "sp"))
    rest_y = first_a[:, 160:]
    first_a = first_a[:, :160]
    first_a, first_b, rest_y = lax.optimization_barrier((first_a, first_b, rest_y))
    own_b = spread(lambda k: along_zy(0, k), first_b, "sp")
    own_a = spread(lambda k: along_zy(k, 0), first_a, "sp")
    rest_z = spread(lambda k: along_zy(k, 0), rest_y, "sp")
    far_a = [lax.ppermute(block, "dp", pairs(1, 8)) for block in own_a]
    far_b = [lax.ppermute(block, "dp", pairs(1, 8)) for block in own_b]
    packed, done = pl.pallas_call(
        project_kernel,
        out_shape=(
            pltpu.VMEM((sp_size, rows + rows // 2, 128), bf),
            jax.ShapeDtypeStruct((8, 128), jnp.float32),
        ),
        in_specs=[VMEM] * (1 + 4 * SIDE),
        out_specs=(VMEM, VMEM),
        scratch_shapes=[pltpu.VMEM((rows, width), bf), pltpu.VMEM((sp_size, 96, rows), jnp.float32)],
        compiler_params=pltpu.CompilerParams(vmem_limit_bytes=30 * 2**20),
        name="project",
    )(*near(normed, *own_a, *own_b, *far_a, *far_b))
    _, rest_z = lax.optimization_barrier((done, rest_z))
    rest_x = spread(along_x, jnp.stack(rest_z), "dp")

    got = lax.all_to_all(packed, "sp", split_axis=0, concat_axis=0, tiled=True)
    gains = lax.dynamic_slice_in_dim(out_gain, sp * HEAD_DIM, HEAD_DIM, 0)[None]
    length = sp_size * rows
    bk = 256
    heads = pl.pallas_call(
        functools.partial(attend_kernel, src=sp_size, rows=rows, bk=bk),
        out_shape=pltpu.VMEM((sp_size, rows // 2, 128), bf),
        in_specs=[VMEM] * 3,
        out_specs=VMEM,
        scratch_shapes=[
            pltpu.VMEM((length, 256), bf),
            pltpu.VMEM((256, length), bf),
            pltpu.VMEM((length, HEAD_DIM), bf),
            pltpu.VMEM((length, HEAD_DIM), jnp.float32),
            pltpu.VMEM((length, 128), jnp.float32),
            pltpu.VMEM((bk, bk), jnp.float32),
            pltpu.VMEM((bk, bk), bf),
        ],
        compiler_params=pltpu.CompilerParams(vmem_limit_bytes=30 * 2**20),
        name="attend",
    )(*near(got, key_bias.reshape(1, length), gains))
    heads, rest_x = lax.optimization_barrier((heads, rest_x))
    own_out = jnp.stack(rest_x)
    far_out = lax.ppermute(own_out, "dp", pairs(1, 8))
    returned = lax.all_to_all(heads, "sp", split_axis=0, concat_axis=0, tiled=True)
    mixed = pl.pallas_call(
        output_kernel,
        out_shape=jax.ShapeDtypeStruct((rows, width), bf),
        in_specs=[VMEM] * 3,
        out_specs=VMEM,
        scratch_shapes=[pltpu.VMEM((rows, sp_size * HEAD_DIM), bf)],
        compiler_params=pltpu.CompilerParams(vmem_limit_bytes=30 * 2**20),
        name="output",
    )(*near(returned, own_out, far_out))
    return mixed[None]


def solution(mesh):
    placed = (
        P("dp", "sp", None),
        P(),
        P("dp", "sp"),
        P("dp", "sp"),
        P("dp", "sp"),
        P("dp", None, "sp"),
        P(),
        P("sp", "dp"),
    )

    return jax.shard_map(
        body, mesh=mesh, in_specs=placed, out_specs=P("dp", "sp", None), check_vma=False
    )
```

```python
import functools
import math

import jax
import jax.numpy as jnp
from jax import lax
from jax.experimental import pallas as pl
from jax.experimental.pallas import tpu as pltpu
from jax.sharding import PartitionSpec as P

HEAD_DIM = 64
LOG2E = math.log2(math.e)
norm_eps = 1e-06
SIDE = 4


VMEM = pl.BlockSpec(memory_space=pltpu.VMEM)


def pairs(step, size):
    return [(i, i ^ step) for i in range(size)]


def along_x(k):
    return [(i, (i + 2 * k) % (2 * SIDE)) for i in range(2 * SIDE)]


def along_zy(dz, dy):
    return [
        (s, ((s // SIDE + dz) % SIDE) * SIDE + (s % SIDE + dy) % SIDE) for s in range(SIDE * SIDE)
    ]


def near(*arrays):
    return [pltpu.with_memory_space_constraint(a, pltpu.VMEM) for a in arrays]


def place_of():
    dp, sp = lax.axis_index("dp"), lax.axis_index("sp")
    return lax.div(dp, 2), lax.rem(dp, 2), lax.div(sp, SIDE), lax.rem(sp, SIDE)


def before(here, there):
    return lax.rem(here + SIDE - there, SIDE)


def project_kernel(normed_ref, *refs):
    own_a, own_b, far_a, far_b = (refs[SIDE * i : SIDE * (i + 1)] for i in range(4))
    out_ref, done_ref, order_ref, sums_ref = refs[4 * SIDE :]
    bf = jnp.bfloat16
    x, c, z, y = place_of()
    rows = normed_ref.shape[0]
    for i in range(SIDE):
        for cc in range(2):
            chunk = 2 * jnp.bitwise_xor(x, i) + jnp.bitwise_xor(c, cc)
            order_ref[:, (2 * i + cc) * 256 : (2 * i + cc + 1) * 256] = normed_ref[
                :, pl.ds(pl.multiple_of(chunk * 256, 256), 256)
            ]
    for kz in range(SIDE):
        parts = []
        for i in range(SIDE):
            for refs_a, refs_b in ((own_a, own_b), (far_a, far_b)):
                if i < 2:
                    several = [refs_a[kz][ky, i] for ky in range(SIDE)]
                else:
                    several = [refs_b[ky][kz, i - 2] for ky in range(SIDE)]
                parts.append(jnp.concatenate(several, axis=0))
        weights = jnp.concatenate(parts, axis=1)
        total = lax.dot_general(
            weights, order_ref[...], (((1,), (1,)), ((), ())), preferred_element_type=jnp.float32
        )
        for ky in range(SIDE):
            sums_ref[SIDE * before(z, kz) + before(y, ky)] = total[96 * ky : 96 * (ky + 1), :]
    half = rows // 2
    for g in range(SIDE):
        key = jnp.concatenate([sums_ref[SIDE * g + j, 64:80, :] for j in range(SIDE)], axis=0)
        value = jnp.concatenate([sums_ref[SIDE * g + j, 80:96, :] for j in range(SIDE)], axis=0)
        turned = value.T.astype(bf)
        for j in range(SIDE):
            h = SIDE * g + j
            both = jnp.concatenate([sums_ref[h, :64, :], key], axis=0)
            out_ref[h, :rows, :] = both.T.astype(bf)
            out_ref[h, rows:, :] = jnp.concatenate([turned[:half], turned[half:]], axis=1)
    done_ref[...] = jnp.zeros_like(done_ref)


def masked(block, mask):
    rows = mask.shape[0]
    first = block[:rows] * mask
    return first if block.shape[0] == rows else jnp.concatenate([first, block[rows:]], axis=0)


def attend_kernel(
    got_ref, bias_ref, gain_ref, out_ref, qa_ref, kt_ref, v_ref, acc_ref, car_ref, mask_ref, tri_ref, *, src, rows, bk
):
    bf = jnp.bfloat16
    half = rows // 2
    length = src * rows
    lane = lax.broadcasted_iota(jnp.int32, (rows, 128), 1)
    ones = jnp.where(lane < 3, 1.0, 0.0).astype(bf)
    step = 2 * rows
    row = lax.broadcasted_iota(jnp.int32, (128, step), 0)

    def prepare(p):
        for b in (2 * p, 2 * p + 1):
            both = got_ref[b, :rows, :]
            wide = both[:, :HEAD_DIM].astype(jnp.float32) * (LOG2E * HEAD_DIM ** -0.5)
            high = wide.astype(bf)
            low = (wide - high.astype(jnp.float32)).astype(bf)
            qa_ref[b * rows : (b + 1) * rows, :128] = jnp.concatenate([high, low], axis=1)
            qa_ref[b * rows : (b + 1) * rows, 128:] = ones
            vv = got_ref[b, rows:, :]
            v_ref[b * rows : b * rows + half, :] = vv[:, :HEAD_DIM]
            v_ref[b * rows + half : (b + 1) * rows, :] = vv[:, HEAD_DIM:]
        pair = jnp.concatenate([got_ref[2 * p, :rows, :], got_ref[2 * p + 1, :rows, :]], axis=0)
        kt = pair.astype(jnp.float32).T[HEAD_DIM:, :].astype(bf)
        at = slice(p * step, (p + 1) * step)
        kt_ref[:HEAD_DIM, at] = kt
        kt_ref[HEAD_DIM : 2 * HEAD_DIM, at] = kt
        b2 = bias_ref[:, at] * LOG2E
        b_high = b2.astype(bf).astype(jnp.float32)
        b_mid = (b2 - b_high).astype(bf).astype(jnp.float32)
        b_low = b2 - b_high - b_mid
        tail = jnp.where(row == 0, b_high, jnp.where(row == 1, b_mid, jnp.where(row == 2, b_low, 0.0)))
        kt_ref[2 * HEAD_DIM :, at] = tail.astype(bf)

    ready = src // 2
    below = lax.broadcasted_iota(jnp.int32, (bk, bk), 0) > lax.broadcasted_iota(jnp.int32, (bk, bk), 1)
    mask_ref[...] = jnp.where(below, 1.0, 0.0)
    tri_ref[...] = jnp.where(below, 1.0, 0.0).astype(bf)
    acc_ref[...] = jnp.zeros_like(acc_ref)
    car_ref[...] = jnp.zeros_like(car_ref)

    for c in reversed(range(length // bk)):
        at = c * bk
        while ready * step > at:
            ready -= 1
            prepare(ready)
        x = jnp.dot(qa_ref[at:, :], kt_ref[:, at : at + bk], preferred_element_type=jnp.float32)
        soft = jnp.maximum(x, jnp.log2(1.0 + jnp.exp2(jnp.minimum(x, 126.0))))
        own = x - soft
        soft = masked(soft, mask_ref[...])
        after = jnp.dot(soft.astype(bf), tri_ref[...], preferred_element_type=jnp.float32)
        a = masked(jnp.exp2(own - after), mask_ref[...])
        carry = car_ref[at:, :]
        here = jnp.dot(a.astype(bf), v_ref[at : at + bk, :], preferred_element_type=jnp.float32)
        acc_ref[at:, :] += here * jnp.exp2(-carry)[:, :HEAD_DIM]
        total = after[:, :128] + soft[:, :128]
        car_ref[at:, :] = carry + jnp.broadcast_to(total[:, :1], carry.shape)

    for b in range(src):
        att = acc_ref[b * rows : (b + 1) * rows, :]
        scaled = att * lax.rsqrt(jnp.mean(att * att, axis=1, keepdims=True) + norm_eps) * gain_ref[...]
        head = scaled.astype(bf)
        out_ref[b] = jnp.concatenate([head[:half], head[half:]], axis=1)


def output_kernel(got_ref, own_ref, far_ref, out_ref, heads_ref):
    x, c, z, y = place_of()
    half = got_ref.shape[1]
    for h in range(SIDE * SIDE):
        block = got_ref[h]
        heads_ref[:half, h * HEAD_DIM : (h + 1) * HEAD_DIM] = block[:, :HEAD_DIM]
        heads_ref[half:, h * HEAD_DIM : (h + 1) * HEAD_DIM] = block[:, HEAD_DIM:]
    for i in range(SIDE):
        for cc, ref in ((0, own_ref), (1, far_ref)):
            parts = [
                ref[i, before(z, zs), before(y, ys)] for zs in range(SIDE) for ys in range(SIDE)
            ]
            mixed = jnp.dot(
                heads_ref[...], jnp.concatenate(parts, axis=0), preferred_element_type=jnp.float32
            )
            chunk = 2 * before(x, i) + jnp.bitwise_xor(c, cc)
            out_ref[:, pl.ds(pl.multiple_of(chunk * 256, 256), 256)] = mixed.astype(jnp.bfloat16)


def body(inputs, in_gain, w_query, w_key, w_value, key_bias, out_gain, w_out):
    bf = jnp.bfloat16
    rows, width = inputs.shape[1], inputs.shape[2]
    sp_size = lax.axis_size("sp")
    sp = lax.axis_index("sp")

    wide = inputs[0].astype(jnp.float32)
    normed = (
        wide * lax.rsqrt(jnp.mean(wide * wide, axis=-1, keepdims=True) + norm_eps) * in_gain
    ).astype(bf)

    def spread(perm_of, a, axis):
        return [a] + [lax.ppermute(a, axis, perm_of(k)) for k in range(1, SIDE)]

    piece = jnp.concatenate([w_query.T, w_key.T, w_value.T], axis=0)
    two = jnp.stack([piece, lax.ppermute(piece, "dp", pairs(2, 8))])
    four = lax.ppermute(two, "dp", pairs(4, 8))
    together = jnp.concatenate([two.reshape(192, 256), w_out], axis=0)
    first_a = spread(lambda k: along_zy(0, k), together, "sp")
    first_a = jnp.stack(first_a)
    first_b = jnp.stack(spread(lambda k: along_zy(k, 0), four, "sp"))
    rest_y = first_a[:, 192:]
    first_a = first_a[:, :192].reshape(SIDE, 2, 96, 256)
    first_a, first_b, rest_y = lax.optimization_barrier((first_a, first_b, rest_y))
    own_b = spread(lambda k: along_zy(0, k), first_b, "sp")
    own_a = spread(lambda k: along_zy(k, 0), first_a, "sp")
    rest_z = spread(lambda k: along_zy(k, 0), rest_y, "sp")
    far_a = [lax.ppermute(block, "dp", pairs(1, 8)) for block in own_a]
    far_b = [lax.ppermute(block, "dp", pairs(1, 8)) for block in own_b]
    packed, done = pl.pallas_call(
        project_kernel,
        out_shape=(
            pltpu.VMEM((sp_size, rows + rows // 2, 128), bf),
            jax.ShapeDtypeStruct((8, 128), jnp.float32),
        ),
        in_specs=[VMEM] * (1 + 4 * SIDE),
        out_specs=(VMEM, VMEM),
        scratch_shapes=[pltpu.VMEM((rows, width), bf), pltpu.VMEM((sp_size, 96, rows), jnp.float32)],
        compiler_params=pltpu.CompilerParams(vmem_limit_bytes=30 * 2**20),
        name="project",
    )(*near(normed, *own_a, *own_b, *far_a, *far_b))
    _, rest_z = lax.optimization_barrier((done, rest_z))
    rest_x = spread(along_x, jnp.stack(rest_z), "dp")

    got = lax.all_to_all(packed, "sp", split_axis=0, concat_axis=0, tiled=True)
    gains = lax.dynamic_slice_in_dim(out_gain, sp * HEAD_DIM, HEAD_DIM, 0)[None]
    length = sp_size * rows
    bk = 256
    heads = pl.pallas_call(
        functools.partial(attend_kernel, src=sp_size, rows=rows, bk=bk),
        out_shape=pltpu.VMEM((sp_size, rows // 2, 128), bf),
        in_specs=[VMEM] * 3,
        out_specs=VMEM,
        scratch_shapes=[
            pltpu.VMEM((length, 256), bf),
            pltpu.VMEM((256, length), bf),
            pltpu.VMEM((length, HEAD_DIM), bf),
            pltpu.VMEM((length, HEAD_DIM), jnp.float32),
            pltpu.VMEM((length, 128), jnp.float32),
            pltpu.VMEM((bk, bk), jnp.float32),
            pltpu.VMEM((bk, bk), bf),
        ],
        compiler_params=pltpu.CompilerParams(vmem_limit_bytes=30 * 2**20),
        name="attend",
    )(*near(got, key_bias.reshape(1, length), gains))
    heads, rest_x = lax.optimization_barrier((heads, rest_x))
    own_out = jnp.stack(rest_x)
    far_out = lax.ppermute(own_out, "dp", pairs(1, 8))
    returned = lax.all_to_all(heads, "sp", split_axis=0, concat_axis=0, tiled=True)
    mixed = pl.pallas_call(
        output_kernel,
        out_shape=jax.ShapeDtypeStruct((rows, width), bf),
        in_specs=[VMEM] * 3,
        out_specs=VMEM,
        scratch_shapes=[pltpu.VMEM((rows, sp_size * HEAD_DIM), bf)],
        compiler_params=pltpu.CompilerParams(vmem_limit_bytes=30 * 2**20),
        name="output",
    )(*near(returned, own_out, far_out))
    return mixed[None]


def solution(mesh):
    placed = (
        P("dp", "sp", None),
        P(),
        P("dp", "sp"),
        P("dp", "sp"),
        P("dp", "sp"),
        P("dp", None, "sp"),
        P(),
        P("sp", "dp"),
    )

    return jax.shard_map(
        body, mesh=mesh, in_specs=placed, out_specs=P("dp", "sp", None), check_vma=False
    )
```

```python
import functools
import math

import jax
import jax.numpy as jnp
from jax import lax
from jax.experimental import pallas as pl
from jax.experimental.pallas import tpu as pltpu
from jax.sharding import PartitionSpec as P

HEAD_DIM = 64
LOG2E = math.log2(math.e)
norm_eps = 1e-06
SIDE = 4


VMEM = pl.BlockSpec(memory_space=pltpu.VMEM)


def pairs(step, size):
    return [(i, i ^ step) for i in range(size)]


def along_x(k):
    return [(i, (i + 2 * k) % (2 * SIDE)) for i in range(2 * SIDE)]


def along_zy(dz, dy):
    return [
        (s, ((s // SIDE + dz) % SIDE) * SIDE + (s % SIDE + dy) % SIDE) for s in range(SIDE * SIDE)
    ]


def near(*arrays):
    return [pltpu.with_memory_space_constraint(a, pltpu.VMEM) for a in arrays]


def place_of():
    dp, sp = lax.axis_index("dp"), lax.axis_index("sp")
    return lax.div(dp, 2), lax.rem(dp, 2), lax.div(sp, SIDE), lax.rem(sp, SIDE)


def before(here, there):
    return lax.rem(here + SIDE - there, SIDE)


def project_kernel(normed_ref, *refs):
    own_a, own_b, far_a, far_b = (refs[SIDE * i : SIDE * (i + 1)] for i in range(4))
    out_ref, done_ref, order_ref, sums_ref = refs[4 * SIDE :]
    bf = jnp.bfloat16
    x, c, z, y = place_of()
    rows = normed_ref.shape[0]
    for i in range(SIDE):
        for cc in range(2):
            chunk = 2 * jnp.bitwise_xor(x, i) + jnp.bitwise_xor(c, cc)
            order_ref[:, (2 * i + cc) * 256 : (2 * i + cc + 1) * 256] = normed_ref[
                :, pl.ds(pl.multiple_of(chunk * 256, 256), 256)
            ]
    for kz in range(SIDE):
        parts = []
        for i in range(SIDE):
            for refs_a, refs_b in ((own_a, own_b), (far_a, far_b)):
                if i < 2:
                    several = [refs_a[kz][ky, i] for ky in range(SIDE)]
                else:
                    several = [refs_b[ky][kz, i - 2] for ky in range(SIDE)]
                parts.append(jnp.concatenate(several, axis=0))
        weights = jnp.concatenate(parts, axis=1)
        total = lax.dot_general(
            weights, order_ref[...], (((1,), (1,)), ((), ())), preferred_element_type=jnp.float32
        )
        for ky in range(SIDE):
            sums_ref[SIDE * before(z, kz) + before(y, ky)] = total[96 * ky : 96 * (ky + 1), :]
    half = rows // 2
    for g in range(SIDE):
        key = jnp.concatenate([sums_ref[SIDE * g + j, 64:80, :] for j in range(SIDE)], axis=0)
        value = jnp.concatenate([sums_ref[SIDE * g + j, 80:96, :] for j in range(SIDE)], axis=0)
        turned = value.T.astype(bf)
        for j in range(SIDE):
            h = SIDE * g + j
            both = jnp.concatenate([sums_ref[h, :64, :], key], axis=0)
            out_ref[h, :rows, :] = both.T.astype(bf)
            out_ref[h, rows:, :] = jnp.concatenate([turned[:half], turned[half:]], axis=1)
    done_ref[...] = jnp.zeros_like(done_ref)


def masked(block, mask):
    rows = mask.shape[0]
    first = block[:rows] * mask
    return first if block.shape[0] == rows else jnp.concatenate([first, block[rows:]], axis=0)


def attend_kernel(
    got_ref, bias_ref, gain_ref, out_ref, qa_ref, kt_ref, v_ref, acc_ref, car_ref, mask_ref, tri_ref, *, src, rows, bk
):
    bf = jnp.bfloat16
    half = rows // 2
    length = src * rows
    lane = lax.broadcasted_iota(jnp.int32, (rows, 128), 1)
    ones = jnp.where(lane < 3, 1.0, 0.0).astype(bf)
    for b in range(src):
        both = got_ref[b, :rows, :]
        wide = both[:, :HEAD_DIM].astype(jnp.float32) * (LOG2E * HEAD_DIM ** -0.5)
        high = wide.astype(bf)
        low = (wide - high.astype(jnp.float32)).astype(bf)
        qa_ref[b * rows : (b + 1) * rows, :128] = jnp.concatenate([high, low], axis=1)
        qa_ref[b * rows : (b + 1) * rows, 128:] = ones
        vv = got_ref[b, rows:, :]
        v_ref[b * rows : b * rows + half, :] = vv[:, :HEAD_DIM]
        v_ref[b * rows + half : (b + 1) * rows, :] = vv[:, HEAD_DIM:]
    step = 2 * rows
    for b in range(src // 2):
        pair = jnp.concatenate([got_ref[2 * b, :rows, :], got_ref[2 * b + 1, :rows, :]], axis=0)
        kt = pair.astype(jnp.float32).T[HEAD_DIM:, :].astype(bf)
        kt_ref[:HEAD_DIM, b * step : (b + 1) * step] = kt
        kt_ref[HEAD_DIM : 2 * HEAD_DIM, b * step : (b + 1) * step] = kt
    b2 = bias_ref[...] * LOG2E
    b_high = b2.astype(bf).astype(jnp.float32)
    b_mid = (b2 - b_high).astype(bf).astype(jnp.float32)
    b_low = b2 - b_high - b_mid
    row = lax.broadcasted_iota(jnp.int32, (128, length), 0)
    tail = jnp.where(row == 0, b_high, jnp.where(row == 1, b_mid, jnp.where(row == 2, b_low, 0.0)))
    kt_ref[2 * HEAD_DIM :, :] = tail.astype(bf)

    below = lax.broadcasted_iota(jnp.int32, (bk, bk), 0) > lax.broadcasted_iota(jnp.int32, (bk, bk), 1)
    mask_ref[...] = jnp.where(below, 1.0, 0.0)
    tri_ref[...] = jnp.where(below, 1.0, 0.0).astype(bf)
    acc_ref[...] = jnp.zeros_like(acc_ref)
    car_ref[...] = jnp.zeros_like(car_ref)

    for c in reversed(range(length // bk)):
        at = c * bk
        x = jnp.dot(qa_ref[at:, :], kt_ref[:, at : at + bk], preferred_element_type=jnp.float32)
        soft = jnp.maximum(x, jnp.log2(1.0 + jnp.exp2(jnp.minimum(x, 126.0))))
        own = x - soft
        soft = masked(soft, mask_ref[...])
        after = jnp.dot(soft.astype(bf), tri_ref[...], preferred_element_type=jnp.float32)
        a = masked(jnp.exp2(own - after), mask_ref[...])
        carry = car_ref[at:, :]
        here = jnp.dot(a.astype(bf), v_ref[at : at + bk, :], preferred_element_type=jnp.float32)
        acc_ref[at:, :] += here * jnp.exp2(-carry)[:, :HEAD_DIM]
        total = after[:, :128] + soft[:, :128]
        car_ref[at:, :] = carry + jnp.broadcast_to(total[:, :1], carry.shape)

    for b in range(src):
        att = acc_ref[b * rows : (b + 1) * rows, :]
        scaled = att * lax.rsqrt(jnp.mean(att * att, axis=1, keepdims=True) + norm_eps) * gain_ref[...]
        head = scaled.astype(bf)
        out_ref[b] = jnp.concatenate([head[:half], head[half:]], axis=1)


def output_kernel(got_ref, own_ref, far_ref, out_ref, heads_ref):
    x, c, z, y = place_of()
    half = got_ref.shape[1]
    for h in range(SIDE * SIDE):
        block = got_ref[h]
        heads_ref[:half, h * HEAD_DIM : (h + 1) * HEAD_DIM] = block[:, :HEAD_DIM]
        heads_ref[half:, h * HEAD_DIM : (h + 1) * HEAD_DIM] = block[:, HEAD_DIM:]
    for i in range(SIDE):
        for cc, ref in ((0, own_ref), (1, far_ref)):
            parts = [
                ref[i, before(z, zs), before(y, ys)] for zs in range(SIDE) for ys in range(SIDE)
            ]
            mixed = jnp.dot(
                heads_ref[...], jnp.concatenate(parts, axis=0), preferred_element_type=jnp.float32
            )
            chunk = 2 * before(x, i) + jnp.bitwise_xor(c, cc)
            out_ref[:, pl.ds(pl.multiple_of(chunk * 256, 256), 256)] = mixed.astype(jnp.bfloat16)


def body(inputs, in_gain, w_query, w_key, w_value, key_bias, out_gain, w_out):
    bf = jnp.bfloat16
    rows, width = inputs.shape[1], inputs.shape[2]
    sp_size = lax.axis_size("sp")
    sp = lax.axis_index("sp")

    wide = inputs[0].astype(jnp.float32)
    normed = (
        wide * lax.rsqrt(jnp.mean(wide * wide, axis=-1, keepdims=True) + norm_eps) * in_gain
    ).astype(bf)

    def spread(perm_of, a, axis):
        return [a] + [lax.ppermute(a, axis, perm_of(k)) for k in range(1, SIDE)]

    piece = jnp.concatenate([w_query.T, w_key.T, w_value.T], axis=0)
    two = jnp.stack([piece, lax.ppermute(piece, "dp", pairs(2, 8))])
    four = lax.ppermute(two, "dp", pairs(4, 8))
    together = jnp.concatenate([two.reshape(192, 256), w_out], axis=0)
    first_a = spread(lambda k: along_zy(0, k), together, "sp")
    first_a = jnp.stack(first_a)
    first_b = jnp.stack(spread(lambda k: along_zy(k, 0), four, "sp"))
    rest_y = first_a[:, 192:]
    first_a = first_a[:, :192].reshape(SIDE, 2, 96, 256)
    first_a, first_b, rest_y = lax.optimization_barrier((first_a, first_b, rest_y))
    own_b = spread(lambda k: along_zy(0, k), first_b, "sp")
    own_a = spread(lambda k: along_zy(k, 0), first_a, "sp")
    rest_z = spread(lambda k: along_zy(k, 0), rest_y, "sp")
    far_a = [lax.ppermute(block, "dp", pairs(1, 8)) for block in own_a]
    far_b = [lax.ppermute(block, "dp", pairs(1, 8)) for block in own_b]
    packed, done = pl.pallas_call(
        project_kernel,
        out_shape=(
            pltpu.VMEM((sp_size, rows + rows // 2, 128), bf),
            jax.ShapeDtypeStruct((8, 128), jnp.float32),
        ),
        in_specs=[VMEM] * (1 + 4 * SIDE),
        out_specs=(VMEM, VMEM),
        scratch_shapes=[pltpu.VMEM((rows, width), bf), pltpu.VMEM((sp_size, 96, rows), jnp.float32)],
        compiler_params=pltpu.CompilerParams(vmem_limit_bytes=30 * 2**20),
        name="project",
    )(*near(normed, *own_a, *own_b, *far_a, *far_b))
    _, rest_z = lax.optimization_barrier((done, rest_z))
    rest_x = spread(along_x, jnp.stack(rest_z), "dp")

    got = lax.all_to_all(packed, "sp", split_axis=0, concat_axis=0, tiled=True)
    gains = lax.dynamic_slice_in_dim(out_gain, sp * HEAD_DIM, HEAD_DIM, 0)[None]
    length = sp_size * rows
    bk = 256
    heads = pl.pallas_call(
        functools.partial(attend_kernel, src=sp_size, rows=rows, bk=bk),
        out_shape=pltpu.VMEM((sp_size, rows // 2, 128), bf),
        in_specs=[VMEM] * 3,
        out_specs=VMEM,
        scratch_shapes=[
            pltpu.VMEM((length, 256), bf),
            pltpu.VMEM((256, length), bf),
            pltpu.VMEM((length, HEAD_DIM), bf),
            pltpu.VMEM((length, HEAD_DIM), jnp.float32),
            pltpu.VMEM((length, 128), jnp.float32),
            pltpu.VMEM((bk, bk), jnp.float32),
            pltpu.VMEM((bk, bk), bf),
        ],
        compiler_params=pltpu.CompilerParams(vmem_limit_bytes=30 * 2**20),
        name="attend",
    )(*near(got, key_bias.reshape(1, length), gains))
    heads, rest_x = lax.optimization_barrier((heads, rest_x))
    own_out = jnp.stack(rest_x)
    far_out = lax.ppermute(own_out, "dp", pairs(1, 8))
    returned = lax.all_to_all(heads, "sp", split_axis=0, concat_axis=0, tiled=True)
    mixed = pl.pallas_call(
        output_kernel,
        out_shape=jax.ShapeDtypeStruct((rows, width), bf),
        in_specs=[VMEM] * 3,
        out_specs=VMEM,
        scratch_shapes=[pltpu.VMEM((rows, sp_size * HEAD_DIM), bf)],
        compiler_params=pltpu.CompilerParams(vmem_limit_bytes=30 * 2**20),
        name="output",
    )(*near(returned, own_out, far_out))
    return mixed[None]


def solution(mesh):
    placed = (
        P("dp", "sp", None),
        P(),
        P("dp", "sp"),
        P("dp", "sp"),
        P("dp", "sp"),
        P("dp", None, "sp"),
        P(),
        P("sp", "dp"),
    )

    return jax.shard_map(
        body, mesh=mesh, in_specs=placed, out_specs=P("dp", "sp", None), check_vma=False
    )
```
